32 devices in a mesh: grp: 2 (over x), sp: 8 (over z, y), tp: 2 (over core).
Axes of the slice: x: 2, y: 2, z: 4, core: 2. Of those that a mesh axis runs over, the one named last changes fastest.
Arguments:
- tokens: bfloat16 [8192, 2048], P(('grp', 'sp', 'tp')), parts along dimension 0, may hold values from -60 to 60
- query_weight: bfloat16 [2048, 1024], P(None, 'tp'), may hold values from -0.125 to 0.125
- key_weight: bfloat16 [2048, 1024], P(None, 'tp'), may hold values from -0.125 to 0.125
- value_weight: bfloat16 [2048, 1024], P(None, 'tp'), may hold values from -0.125 to 0.125
- output_weight: bfloat16 [1024, 2048], P(None, 'tp'), may hold values from -1.5 to 1.5
Outputs:
- attended: bfloat16 [8192, 2048], P(('grp', 'sp'), 'tp'), parts along dimension 0
The draws below stay inside these ranges and needn't reach their ends.
There are 2 independent parts, one for each index of `grp`. The reference program is written for one: setup_inputs(seed, part) draws one part's arguments, and reference() takes and returns one part's arrays. A program takes and returns all parts, laid end to end along the dimension named above; an argument that names none is the same for every part. Nothing has to cross between parts.
All inputs are finite; a program needn't handle non-finite values.
Results may differ from the reference program's by a relative error of at most 0.012.
The reference program's roundings to bfloat16 on the way (of `queries`, `keys`, `values`, `weights` and `mixed`) count: a program that leaves them out, or rounds other values in their place, can miss the bound.
Values may be sent and summed in bfloat16 or wider, within the bound.
A program may use at most 128 MiB of HBM per device.

```python
import jax
import jax.numpy as jnp
from jax import lax

D = 2048
HEADS = 8
HEAD = 128
REACH_STEPS = 128
MIDDLE_DILATION = 4
FAR_DILATION = 16
TOKENS = 4096


def draw_tokens(key, part):
    key_base = jax.random.fold_in(key, 11)
    base = jnp.clip(jax.random.normal(key_base, (TOKENS, D), jnp.float32), -6.0, 6.0)
    return base.astype(jnp.bfloat16)


def steps_of(rng, shape, cuts, smallest, largest):
    gain, own = 1.0, jax.random.fold_in(rng, 6)
    for position, blocks in cuts:
        draws = jnp.exp(jax.random.uniform(jax.random.fold_in(own, position), (blocks,), jnp.float32, smallest / len(cuts), largest / len(cuts)))
        gain = gain * jnp.repeat(draws, shape[position] // blocks).reshape([-1 if axis == position else 1 for axis in range(len(shape))])
    return gain


def gaussian(key, extent, deviation, reach, shards=(), kind=jnp.bfloat16):
    factor_of = steps_of(key, extent, shards, -0.22, 0.18) if shards else 1.0
    entries = jax.random.normal(key, extent, jnp.float32) * deviation * factor_of
    return jnp.minimum(jnp.maximum(entries, -reach), reach).astype(kind)


def setup_inputs(seed: int = 0, part: int = 0) -> dict:
    key_of = jax.random.split(jax.random.key(seed), 6)
    own_keys = jax.random.split(jax.random.fold_in(key_of[5], part), 6)
    tokens = draw_tokens(jax.random.fold_in(jax.random.fold_in(key_of[5], part), 71), part)
    query_weight = gaussian(key_of[1], (D, HEADS * HEAD), D ** -0.5, 0.125, ((1, 2),))
    key_weight = gaussian(key_of[2], (D, HEADS * HEAD), D ** -0.5, 0.125, ((1, 2),))
    value_weight = gaussian(key_of[3], (D, HEADS * HEAD), D ** -0.5, 0.125, ((1, 2),))
    output_weight = gaussian(key_of[4], (HEADS * HEAD, D), (REACH_STEPS // 8) ** -0.5, 1.5, ((1, 2),))
    return dict(tokens=tokens, query_weight=query_weight, key_weight=key_weight, value_weight=value_weight, output_weight=output_weight)


THETA_BASE = 500000.0


def rotate(values, positions):
    half = values.shape[-1] // 2
    inverse = THETA_BASE ** (-jnp.arange(half, dtype=jnp.float32) / half)
    angles = positions[:, None, None] * inverse
    cosine = jnp.cos(angles)
    sine = jnp.sin(angles)
    first = values[..., :half]
    second = values[..., half:]
    return jnp.concatenate([first * cosine - second * sine, second * cosine + first * sine], axis=-1)


def pattern(queries, keys, values, pattern_dilation):
    length = queries.shape[0]
    unit = pattern_dilation * REACH_STEPS
    padded = -(-length // unit) * unit
    blocks = padded // unit

    def regroup(array):
        array = jnp.pad(array, ((0, padded - length), (0, 0), (0, 0)))
        return array.reshape(blocks, REACH_STEPS, pattern_dilation, HEADS, HEAD).astype(jnp.float32)

    def with_prev(array):
        earlier = jnp.pad(array, ((1, 0), (0, 0), (0, 0), (0, 0), (0, 0)))[:-1]
        return jnp.concatenate([earlier, array], axis=1)

    query_sub = regroup(queries)
    key_sub = with_prev(regroup(keys))
    value_sub = with_prev(regroup(values))
    scores = jnp.einsum('nqrhd,nkrhd->nrhqk', query_sub, key_sub) * HEAD ** -0.5
    query_index = jnp.arange(REACH_STEPS)[:, None] + REACH_STEPS
    key_index = jnp.arange(2 * REACH_STEPS)[None, :]
    distance = query_index - key_index
    key_global = jnp.arange(blocks)[:, None, None] * REACH_STEPS + key_index[None] - REACH_STEPS
    allowed = ((distance >= 0) & (distance <= REACH_STEPS))[None] & (key_global >= 0)
    scores = jnp.where(allowed[:, None, None], scores, -jnp.inf)
    top = jnp.max(scores, axis=-1, keepdims=True)
    offset_keys = jnp.exp(scores - top)
    total = jnp.sum(offset_keys, axis=-1, keepdims=True)
    weights = lax.optimization_barrier((offset_keys / total).astype(jnp.bfloat16)).astype(jnp.float32)
    result = jnp.einsum('nrhqk,nkrhd->nqrhd', weights, value_sub).reshape(padded, HEADS, HEAD)[:length]
    lse = jnp.transpose((top + jnp.log(total))[..., 0], (0, 3, 1, 2)).reshape(padded, HEADS)[:length]
    return result, lse


def reference(tokens, query_weight, key_weight, value_weight, output_weight):
    length = tokens.shape[0]
    positions = jnp.arange(length).astype(jnp.float32)
    query_proj = jnp.dot(tokens, query_weight, preferred_element_type=jnp.float32).reshape(length, HEADS, HEAD)
    key_proj = jnp.dot(tokens, key_weight, preferred_element_type=jnp.float32).reshape(length, HEADS, HEAD)
    queries = rotate(query_proj, positions).astype(jnp.bfloat16)
    keys = rotate(key_proj, positions).astype(jnp.bfloat16)
    values = jnp.dot(tokens, value_weight, preferred_element_type=jnp.float32).astype(jnp.bfloat16)
    values = values.reshape(length, HEADS, HEAD)
    results = []
    lses = []
    for pattern_dilation in (1, MIDDLE_DILATION, FAR_DILATION):
        result, lse = pattern(queries, keys, values, pattern_dilation)
        results.append(result)
        lses.append(lse)
    mixing = jax.nn.softmax(jnp.stack(lses, axis=0), axis=0)
    mixed = jnp.sum(mixing[..., None] * jnp.stack(results, axis=0), axis=0)
    mixed = mixed.astype(jnp.bfloat16).reshape(length, HEADS * HEAD)
    return jnp.dot(mixed, output_weight, preferred_element_type=jnp.float32).astype(jnp.bfloat16)
```

```python
import functools

import jax
import jax.numpy as jnp
import numpy as np
from jax import lax
from jax.experimental import pallas as pl
from jax.experimental.pallas import tpu as pltpu
from jax.sharding import PartitionSpec as P

HEAD = 128
REACH_STEPS = 128
MIDDLE_DILATION = 4
FAR_DILATION = 16
THETA_BASE = 500000.0
NEG = -1e30
MESH = pl.DeviceIdType.MESH
F32 = jnp.float32
BF16 = jnp.bfloat16

A, C, O = 0, 1, 2
SLOTS = 3
CLASSES = MIDDLE_DILATION
CLASS_ROWS = 128


def spot(i):
    return (i >> 6) * 256 + (i & 15) * 16 + ((i >> 4) & 3) * 4


def iota(shape, dim):
    return lax.broadcasted_iota(jnp.int32, shape, dim)


def rotated(x, cosine, sine):
    return x * cosine + pltpu.roll(x, HEAD // 2, 1) * sine


def softmax(scores, values):
    top = jnp.max(scores, axis=-1, keepdims=True)
    raised = jnp.exp(scores - top)
    total = jnp.sum(raised, axis=-1, keepdims=True)
    weights = (raised * (1.0 / total)).astype(BF16)
    result = jnp.dot(weights, values, preferred_element_type=F32)
    return result, top + jnp.log(total)


def transposed_dot(a, b):
    return lax.dot_general(a, b, (((1,), (1,)), ((), ())), preferred_element_type=F32)


def kernel(
    n_sp, heads,
    tok_hbm, wq_hbm, wk_hbm, wv_hbm, wo_hbm, inv_hbm,
    out_ref,
    tok, wkv, wq, wo, inv, cos_ref, sin_ref, xg, ctx, q, visitor, k1, v1, perm, unperm,
    b16, b4, b1, near_out, near_lse, part, part_lse, far_out, far_lse, mixp, mixg, out_sum,
    load_sem, x_sem, ctx_send, ctx_recv, q_sem, part_sem, lse_sem, mix_send, mix_recv,
):
    sp = lax.axis_index("sp")
    tp = lax.axis_index("tp")
    z = sp // 2
    odd = sp % 2
    even = odd == 0
    other = 1 - tp
    has_next = z + 1 < n_sp // 2

    tok_copy = pltpu.make_async_copy(tok_hbm, tok, load_sem.at[0])
    tok_copy.start()
    inv_copy = pltpu.make_async_copy(inv_hbm, inv, load_sem.at[2 + 2 * heads + heads // 2])
    inv_copy.start()
    kv_copies = []
    for h in range(heads):
        cols = pl.ds(h * HEAD, HEAD)
        pair = (
            pltpu.make_async_copy(wk_hbm.at[:, cols], wkv.at[h, :, pl.ds(0, HEAD)], load_sem.at[1 + 2 * h]),
            pltpu.make_async_copy(wv_hbm.at[:, cols], wkv.at[h, :, pl.ds(HEAD, HEAD)], load_sem.at[2 + 2 * h]),
        )
        for copy in pair:
            copy.start()
        kv_copies.append(pair)
    q_copies = []
    for p in range(heads // 2):
        copy = pltpu.make_async_copy(
            wq_hbm.at[:, pl.ds(p * 2 * HEAD, 2 * HEAD)], wq.at[p], load_sem.at[1 + 2 * heads + p])
        copy.start()
        q_copies.append(copy)
    wo_copy = pltpu.make_async_copy(wo_hbm, wo, load_sem.at[1 + 2 * heads + heads // 2])
    wo_copy.start()

    barrier = pltpu.get_barrier_semaphore()
    y_partner = sp + 1 - 2 * odd

    def greet(ids):
        pl.semaphore_signal(barrier, inc=1, device_id=ids, device_id_type=MESH)

    greet({"tp": other})
    greet({"sp": y_partner})

    @pl.when(has_next)
    def _():
        greet({"sp": sp + 2})

    @pl.when(z > 0)
    def _():
        greet({"sp": sp - 2})

    row = iota((256, 256), 0)
    perm[...] = jnp.where(spot(row & 63) + (row >> 6) == iota((256, 256), 1), 1.0, 0.0).astype(BF16)

    pl.semaphore_wait(barrier, 2 + has_next.astype(jnp.int32) + (z > 0).astype(jnp.int32))

    tok_copy.wait()
    width = tok.shape[1]

    def reorder(i, _):
        cols = pl.ds(pl.multiple_of(i * 512, 512), 512)
        moved = jnp.dot(perm[...], tok[:, cols], preferred_element_type=F32).astype(BF16)
        xg[:, tp, :, cols] = moved.reshape(CLASSES, 64, 512)
        return 0

    lax.fori_loop(0, width // 512, reorder, 0)
    x_copy = pltpu.make_async_remote_copy(
        src_ref=xg.at[:, tp], dst_ref=xg.at[:, tp], send_sem=x_sem.at[0], recv_sem=x_sem.at[1],
        device_id={"tp": other}, device_id_type=MESH)
    x_copy.start()

    inv_copy.wait()
    lane = iota((128, HEAD), 1)

    def table(c, _):
        positions = sp * 512 + spot(iota((128, HEAD), 0)) + c
        angles = positions.astype(F32) * inv[...]
        rows = pl.ds(pl.multiple_of(c * 128, 128), 128)
        cos_ref[rows, :] = jnp.cos(angles)
        sine = jnp.sin(angles)
        sin_ref[rows, :] = jnp.where(lane < HEAD // 2, -sine, sine)
        return 0

    lax.fori_loop(0, CLASSES, table, 0)

    def remote(src, dst, send_sem, recv_sem, ids):
        return pltpu.make_async_remote_copy(
            src_ref=src, dst_ref=dst, send_sem=send_sem, recv_sem=recv_sem,
            device_id=ids, device_id_type=MESH)

    down = {"sp": sp + 2}
    up = {"sp": sp - 2}
    side = {"sp": y_partner}

    def send(h, src, dst, ids):
        return remote(ctx.at[h, :, :, src], ctx.at[h, :, :, dst],
                      ctx_send.at[dst, h], ctx_recv.at[dst, h], ids)

    def send_own(h):
        return ((has_next, send(h, O, A, down)), (even, send(h, O, C, side)))

    def send_relay(h):
        return (((odd == 1) & (z > 0), send(h, A, C, side)),)

    def send_query(h):
        return ((z > 0, remote(q.at[h], visitor.at[h], q_sem.at[0, h], q_sem.at[1, h], up)),)

    def send_part(h):
        return ((has_next, remote(part.at[h], far_out.at[h], part_sem.at[0, h], part_sem.at[1, h], down)),
                (has_next, remote(part_lse.at[h], far_lse.at[h], lse_sem.at[0, h], lse_sem.at[1, h], down)))

    def start_all(sends):
        for condition, copy in sends:
            @pl.when(condition)
            def _():
                copy.start()

    def receive(h, slot):
        @pl.when(sp >= 2 - slot)
        def _():
            send(h, slot, slot, side).wait_recv()

    x_copy.wait_recv()

    def tokens():
        return xg[...].reshape(512, width)

    def project_kv(h, _):
        kv = jnp.dot(tokens(), wkv[h], preferred_element_type=F32)
        k = rotated(kv[:, :HEAD], cos_ref[...], sin_ref[...]).astype(BF16)
        ctx[h, 0, :, O] = k.reshape(CLASSES, 128, HEAD)
        ctx[h, 1, :, O] = kv[:, HEAD:].astype(BF16).reshape(CLASSES, 128, HEAD)
        start_all(send_own(h))
        return 0

    for pair in kv_copies:
        for copy in pair:
            copy.wait()
    lax.fori_loop(0, heads, project_kv, 0)

    for copy in q_copies:
        copy.wait()

    def project_q(p, _):
        qq = jnp.dot(tokens(), wq[p], preferred_element_type=F32)
        for s in range(2):
            r = rotated(qq[:, s * HEAD:(s + 1) * HEAD], cos_ref[...], sin_ref[...])
            q[2 * p + s] = r.astype(BF16).reshape(CLASSES, 128, HEAD)
            start_all(send_query(2 * p + s))
        return 0

    lax.fori_loop(0, heads // 2, project_q, 0)

    qi, kj = iota((128, 640), 0), iota((128, 640), 1)
    dist = 4 - (kj >> 7)
    diff = spot(qi) - spot(kj & 127) + 512 * dist
    here = (dist <= sp) | ((dist >= 3) & (dist <= sp + 2))
    far = here & ((diff & 15) == 0) & (diff >= 0) & (diff <= FAR_DILATION * REACH_STEPS)
    b16[...] = jnp.where(far, 0.0, NEG)
    mid = here & (diff >= 0) & (diff <= MIDDLE_DILATION * REACH_STEPS)
    b4[...] = jnp.where(mid, 0.0, NEG)[:, 384:]
    key_spot = jnp.where(kj < 128, kj - 128, spot(kj & 127) + ((kj >> 7) - 1))
    for c in range(CLASSES):
        near = spot(qi) + c - key_spot
        ok = (near >= 0) & (near <= REACH_STEPS) & ((kj >= 128) | (sp > 0))
        b1[c] = jnp.where(ok, 0.0, NEG)
    col = iota((512, 512), 1)
    unperm[...] = jnp.where(spot(col & 127) + (col >> 7) == iota((512, 512), 0), 1.0, 0.0).astype(BF16)

    for slot in (A, C):
        @pl.when(sp < 2 - slot)
        def _():
            def clear(h, _):
                ctx[h, :, :, slot] = jnp.zeros((2, CLASSES, 128, HEAD), BF16)
                return 0
            lax.fori_loop(0, heads, clear, 0)

    part_lse[...] = jnp.zeros(part_lse.shape, F32)

    @pl.when(z == 0)
    def _():
        far_out[...] = jnp.zeros(far_out.shape, BF16)
        far_lse[...] = jnp.full(far_lse.shape, NEG, F32)

    def mix_copy(h):
        cols = pl.ds(pl.multiple_of(h * HEAD, HEAD), HEAD)
        return pltpu.make_async_remote_copy(
            src_ref=mixg.at[tp, :, cols], dst_ref=mixg.at[tp, :, cols],
            send_sem=mix_send.at[h], recv_sem=mix_recv.at[h],
            device_id={"tp": other}, device_id_type=MESH)

    eye = iota((128, 128), 0) == iota((128, 128), 1)

    def visit(h):
        @pl.when(has_next)
        def _():
            remote(q.at[h], visitor.at[h], q_sem.at[0, h], q_sem.at[1, h], side).wait_recv()

            def of_class(c, _):
                keys = ctx[h, 0, c, A:O].reshape(2 * 128, HEAD)
                vals = ctx[h, 1, c, A:O].reshape(2 * 128, HEAD)
                scores = transposed_dot(visitor[h, c], keys) * HEAD ** (-0.5)
                result, lse = softmax(scores + b16[:, :256], vals)
                part[h, c] = result.astype(BF16)
                part_lse[h, pl.ds(c, 1), :] = jnp.sum(jnp.where(eye, lse, 0.0), axis=0, keepdims=True)
                return 0

            lax.fori_loop(0, CLASSES, of_class, 0)

        start_all(send_part(h))

    def attend(h):
        tail = unperm[384:512, :]
        for kv, near in ((0, k1), (1, v1)):
            last = ctx[h, kv, :, C].reshape(512, HEAD)
            near[0:128] = jnp.dot(tail, last, preferred_element_type=F32).astype(BF16)
            near[128:640] = ctx[h, kv, :, O].reshape(512, HEAD)

        def of_class(c, _):
            qc = q[h, c]
            keys = ctx[h, 0, c].reshape(SLOTS * 128, HEAD)
            vals = ctx[h, 1, c].reshape(SLOTS * 128, HEAD)
            scores = transposed_dot(qc, keys) * HEAD ** (-0.5)
            r16, l16 = softmax(scores + b16[:, 256:], vals)
            r4, l4 = softmax(scores[:, 128:] + b4[...], vals[128:])
            r1, l1 = softmax(transposed_dot(qc, k1[...]) * HEAD ** (-0.5) + b1[c], v1[...])
            most = jnp.maximum(jnp.maximum(l16, l4), l1)
            e16, e4, e1 = jnp.exp(l16 - most), jnp.exp(l4 - most), jnp.exp(l1 - most)
            total = e16 + e4 + e1
            share = 1.0 / total
            near_out[h, c] = r1 * (e1 * share) + r4 * (e4 * share) + r16 * (e16 * share)
            near_lse[h, c] = jnp.broadcast_to(most + jnp.log(total), (128, HEAD))
            return 0

        lax.fori_loop(0, CLASSES, of_class, 0)

    def step(h, _):
        @pl.when(h < heads)
        def _():
            receive(h, A)
            start_all(send_relay(h))

        @pl.when(h > 0)
        def _():
            receive(h - 1, C)
            visit(h - 1)

        @pl.when((h > 0) & (h < heads))
        def _():
            attend(h - 1)
        return 0

    lax.fori_loop(0, heads + 1, step, 0)

    def combine(h):
        @pl.when(z > 0)
        def _():
            remote(part.at[h], far_out.at[h], part_sem.at[0, h], part_sem.at[1, h], side).wait_recv()
            remote(part_lse.at[h], far_lse.at[h], lse_sem.at[0, h], lse_sem.at[1, h], side).wait_recv()

        for c in range(CLASSES):
            row = far_lse[h, c:c + 1, :]
            lf = jnp.sum(jnp.where(eye, row, 0.0), axis=1, keepdims=True)
            ln = near_lse[h, c]
            most = jnp.maximum(ln, lf)
            en, ef = jnp.exp(ln - most), jnp.exp(lf - most)
            mixed = (near_out[h, c] * en + far_out[h, c].astype(F32) * ef) / (en + ef)
            mixp[c * 128:(c + 1) * 128, :] = mixed.astype(BF16)
        natural = jnp.dot(unperm[...], mixp[...], preferred_element_type=F32).astype(BF16)
        cols = pl.ds(pl.multiple_of(h * HEAD, HEAD), HEAD)
        mixg[tp, :, cols] = natural
        mix_copy(h).start()

    def gathered(h, _):
        mix_copy(h).wait_recv()
        return 0

    half = mixg.shape[2]
    first = half // 2

    def partial_out(i, _):
        cols = pl.ds(pl.multiple_of(i * 256, 256), 256)
        total = jnp.dot(mixg[0, :, :first], wo[:first, cols], preferred_element_type=F32)
        total = total + jnp.dot(mixg[1, :, :first], wo[half:half + first, cols], preferred_element_type=F32)
        out_sum[:, cols] = total
        return 0

    def finish(h, _):
        @pl.when(h == heads - 2)
        def _():
            attend(heads - 1)

        @pl.when(h == heads - 1)
        def _():
            wo_copy.wait()
            lax.fori_loop(0, heads // 2, gathered, 0)
            lax.fori_loop(0, out_ref.shape[1] // 256, partial_out, 0)

        combine(h)
        return 0

    lax.fori_loop(0, heads, finish, 0)

    lax.fori_loop(heads // 2, heads, gathered, 0)

    def project_out(i, _):
        cols = pl.ds(pl.multiple_of(i * 256, 256), 256)
        total = jnp.dot(mixg[0, :, first:], wo[first:half, cols], preferred_element_type=F32)
        total = total + jnp.dot(mixg[1, :, first:], wo[half + first:, cols], preferred_element_type=F32)
        out_ref[:, cols] = (out_sum[:, cols] + total).astype(BF16)
        return 0

    lax.fori_loop(0, out_ref.shape[1] // 256, project_out, 0)

    x_copy.wait_send()

    def left(h, _):
        for sends in (send_own(h), send_relay(h), send_query(h), send_part(h)):
            for condition, copy in sends:
                @pl.when(condition)
                def _():
                    copy.wait_send()
        mix_copy(h).wait_send()
        return 0

    lax.fori_loop(0, heads, left, 0)


def body(tokens, query_weight, key_weight, value_weight, output_weight):
    n_sp = lax.axis_size("sp")
    half_rows, width = tokens.shape
    rows = half_rows * lax.axis_size("tp")
    heads = query_weight.shape[1] // HEAD
    assert rows * 4 == FAR_DILATION * REACH_STEPS and rows == 512
    assert n_sp % 2 == 0 and lax.axis_size("tp") == 2 and heads % 2 == 0 and heads >= 4

    half = HEAD // 2
    inverse = THETA_BASE ** (-np.arange(half, dtype=np.float64) / half)
    inverse = np.concatenate([inverse, inverse]).astype(np.float32)[None, :]

    anywhere = pl.BlockSpec(memory_space=pl.ANY)
    vmem = pl.BlockSpec(memory_space=pltpu.VMEM)
    out_cols = output_weight.shape[1]
    return pl.pallas_call(
        functools.partial(kernel, n_sp, heads),
        out_shape=pltpu.VMEM((rows, out_cols), BF16),
        in_specs=[anywhere] * 6,
        out_specs=vmem,
        scratch_shapes=[
            pltpu.VMEM((half_rows, width), BF16),
            pltpu.VMEM((heads, width, 2 * HEAD), BF16),
            pltpu.VMEM((heads // 2, width, 2 * HEAD), BF16),
            pltpu.VMEM(output_weight.shape, BF16),
            pltpu.VMEM((1, HEAD), F32),
            pltpu.VMEM((rows, HEAD), F32),
            pltpu.VMEM((rows, HEAD), F32),
            pltpu.VMEM((CLASSES, 2, 64, width), BF16),
            pltpu.VMEM((heads, 2, CLASSES, SLOTS, 128, HEAD), BF16),
            pltpu.VMEM((heads, CLASSES, 128, HEAD), BF16),
            pltpu.VMEM((heads, CLASSES, 128, HEAD), BF16),
            pltpu.VMEM((640, HEAD), BF16),
            pltpu.VMEM((640, HEAD), BF16),
            pltpu.VMEM((256, 256), BF16),
            pltpu.VMEM((512, 512), BF16),
            pltpu.VMEM((128, 640), F32),
            pltpu.VMEM((128, 256), F32),
            pltpu.VMEM((CLASSES, 128, 640), F32),
            pltpu.VMEM((heads, CLASSES, 128, HEAD), F32),
            pltpu.VMEM((heads, CLASSES, 128, HEAD), F32),
            pltpu.VMEM((heads, CLASSES, 128, HEAD), BF16),
            pltpu.VMEM((heads, 8, 128), F32),
            pltpu.VMEM((heads, CLASSES, 128, HEAD), BF16),
            pltpu.VMEM((heads, 8, 128), F32),
            pltpu.VMEM((512, HEAD), BF16),
            pltpu.VMEM((2, rows, heads * HEAD), BF16),
            pltpu.VMEM((rows, out_cols), F32),
            pltpu.SemaphoreType.DMA((3 + 2 * heads + heads // 2,)),
            pltpu.SemaphoreType.DMA((2,)),
            pltpu.SemaphoreType.DMA((2, heads)),
            pltpu.SemaphoreType.DMA((2, heads)),
            pltpu.SemaphoreType.DMA((2, heads)),
            pltpu.SemaphoreType.DMA((2, heads)),
            pltpu.SemaphoreType.DMA((2, heads)),
            pltpu.SemaphoreType.DMA((heads,)),
            pltpu.SemaphoreType.DMA((heads,)),
        ],
        compiler_params=pltpu.CompilerParams(
            collective_id=0, has_side_effects=True, vmem_limit_bytes=56 * 1024 * 1024
        ),
    )(tokens, query_weight, key_weight, value_weight, output_weight, jnp.asarray(inverse))


def solution(mesh):
    in_specs = (
        P(("grp", "sp", "tp"), None),
        P(None, "tp"),
        P(None, "tp"),
        P(None, "tp"),
        P(None, "tp"),
    )
    out_specs = P(("grp", "sp"), "tp")
    return jax.shard_map(body, mesh=mesh, in_specs=in_specs, out_specs=out_specs, check_vma=False)
```

```python
import functools

import jax
import jax.numpy as jnp
import numpy as np
from jax import lax
from jax.experimental import pallas as pl
from jax.experimental.pallas import tpu as pltpu
from jax.sharding import PartitionSpec as P

HEAD = 128
REACH_STEPS = 128
MIDDLE_DILATION = 4
FAR_DILATION = 16
THETA_BASE = 500000.0
NEG = -1e30
MESH = pl.DeviceIdType.MESH
F32 = jnp.float32
BF16 = jnp.bfloat16
SCALE = HEAD ** -0.5 / float(np.log(2.0))

A, C, O = 0, 1, 2
SLOTS = 3
CLASSES = MIDDLE_DILATION
PIECES = 2


def iota(shape, dim):
    return lax.broadcasted_iota(jnp.int32, shape, dim)


def rotated(x, cosine, sine):
    return x * cosine + pltpu.roll(x, HEAD // 2, 1) * sine


def weighed(scores, values):
    top = jnp.max(scores, axis=-1, keepdims=True)
    raised = jnp.exp2(scores - top).astype(BF16)
    ones = jnp.ones(values.shape, BF16)
    both = jnp.dot(raised, jnp.concatenate([values, ones], axis=1), preferred_element_type=F32)
    return both[:, :HEAD], both[:, HEAD:], top


def transposed_dot(a, b):
    return lax.dot_general(a, b, (((1,), (1,)), ((), ())), preferred_element_type=F32)


def classed(start, count, c):
    return pl.ds(start + c, count, stride=CLASSES)


def kernel(
    n_sp, heads,
    tok_hbm, wq_hbm, wk_hbm, wv_hbm, wo_hbm, inv_hbm,
    out_ref,
    x, wkv, wq, wo, inv, cos_ref, sin_ref, ctx, q, qn, kn, vn, visitor, flat_a, flat_b,
    far_bias, visit_bias, band, num, tot, top, cnum, ctot, ctop,
    part, part_lse, far_out, far_lse, mixf, mixg, out_sum,
    tok_sem, kv_sem, q_load, wo_sem, inv_sem, x_send, x_recv,
    ctx_send, ctx_recv, q_sem, part_sem, lse_sem, mix_send, mix_recv,
):
    sp = lax.axis_index("sp")
    tp = lax.axis_index("tp")
    z = sp // 2
    odd = sp % 2
    even = odd == 0
    other = 1 - tp
    has_next = z + 1 < n_sp // 2
    half_rows = x.shape[1]
    rows = 2 * half_rows
    class_rows = rows // CLASSES
    half_class = class_rows // 2
    piece = half_rows // PIECES
    order = (tp, other)

    tok_copies = []
    for i in range(PIECES):
        span = pl.ds(i * piece, piece)
        copy = pltpu.make_async_copy(tok_hbm.at[span], x.at[tp, span], tok_sem.at[i])
        copy.start()
        tok_copies.append(copy)
    inv_copy = pltpu.make_async_copy(inv_hbm, inv, inv_sem.at[0])
    inv_copy.start()

    def kv_copy(h, kind):
        source = (wk_hbm, wv_hbm)[kind]
        cols = pl.ds(h * HEAD, HEAD)
        return pltpu.make_async_copy(source.at[:, cols], wkv.at[h, :, pl.ds(kind * HEAD, HEAD)], kv_sem.at[kind, h])

    for h in range(heads):
        for kind in range(2):
            kv_copy(h, kind).start()
    q_copies = []
    for p in range(heads // 2):
        copy = pltpu.make_async_copy(wq_hbm.at[:, pl.ds(p * 2 * HEAD, 2 * HEAD)], wq.at[p], q_load.at[p])
        copy.start()
        q_copies.append(copy)
    wo_copies = []
    for h in range(heads):
        for t in range(2):
            copy = pltpu.make_async_copy(
                wo_hbm.at[pl.ds((t * heads + h) * HEAD, HEAD)], wo.at[pl.ds((2 * h + t) * HEAD, HEAD)], wo_sem.at[t, h])
            copy.start()
            wo_copies.append(copy)

    barrier = pltpu.get_barrier_semaphore()
    y_partner = sp + 1 - 2 * odd

    def greet(ids):
        pl.semaphore_signal(barrier, inc=1, device_id=ids, device_id_type=MESH)

    greet({"tp": other})
    greet({"sp": y_partner})

    @pl.when(has_next)
    def _():
        greet({"sp": sp + 2})

    @pl.when(z > 0)
    def _():
        greet({"sp": sp - 2})

    def remote(src, dst, send_sem, recv_sem, ids):
        return pltpu.make_async_remote_copy(
            src_ref=src, dst_ref=dst, send_sem=send_sem, recv_sem=recv_sem,
            device_id=ids, device_id_type=MESH)

    down = {"sp": sp + 2}
    up = {"sp": sp - 2}
    side = {"sp": y_partner}
    across = {"tp": other}

    block = REACH_STEPS
    qi, kj = iota((block, SLOTS * block), 0), iota((block, SLOTS * block), 1)
    dist = O - kj // block
    steps = qi - (kj % block) + block * dist
    here = dist <= sp
    ratio = FAR_DILATION // MIDDLE_DILATION
    mid = here & (steps >= 0) & (steps <= REACH_STEPS)
    far = here & (steps >= 0) & (steps % ratio == 0) & (steps <= ratio * REACH_STEPS)
    far_bias[...] = jnp.where(mid & far, 1.0, jnp.where(mid | far, 0.0, NEG))
    older = steps[:, :2 * block] + 2 * block
    seen = here[:, :2 * block] & (older % ratio == 0) & (older <= ratio * REACH_STEPS)
    visit_bias[...] = jnp.where(seen, 0.0, NEG)
    ni, nj = iota((block, 2 * block), 0), iota((block, 2 * block), 1)
    gap = ni + block - nj
    band[1] = jnp.where((gap >= 0) & (gap <= REACH_STEPS), 0.0, NEG)
    share = block // CLASSES
    tail_gap = ni + block - ((nj % share) * CLASSES + nj // share)
    gap = jnp.where(nj < block, tail_gap, gap)
    band[0] = jnp.where((gap >= 0) & (gap <= REACH_STEPS) & ((nj >= block) | (sp > 0)), 0.0, NEG)

    for slot in (A, C):
        @pl.when(sp < 2 - slot)
        def _():
            def clear(h, _):
                ctx[h, :, :, slot] = jnp.zeros((2, CLASSES, class_rows, HEAD), BF16)
                return 0
            lax.fori_loop(0, heads, clear, 0)

    part_lse[...] = jnp.zeros(part_lse.shape, F32)

    @pl.when(z == 0)
    def _():
        far_out[...] = jnp.zeros(far_out.shape, BF16)
        far_lse[...] = jnp.full(far_lse.shape, NEG, F32)

    lane = iota((piece, HEAD), 1)

    def table(c, _):
        start = pl.multiple_of(c * piece, piece)
        positions = sp * rows + start + iota((piece, HEAD), 0)
        angles = positions.astype(F32) * inv[...]
        span = pl.ds(start, piece)
        cos_ref[span, :] = jnp.cos(angles)
        sine = jnp.sin(angles)
        sin_ref[span, :] = jnp.where(lane < HEAD // 2, -sine, sine)
        return 0

    inv_copy.wait()
    lax.fori_loop(tp * PIECES, tp * PIECES + PIECES, table, 0)

    pl.semaphore_wait(barrier, 2 + has_next.astype(jnp.int32) + (z > 0).astype(jnp.int32))

    def x_copy(i):
        span = pl.ds(i * piece, piece)
        return remote(x.at[tp, span], x.at[tp, span], x_send.at[i], x_recv.at[i], across)

    for i in range(PIECES):
        tok_copies[i].wait()
        x_copy(i).start()

    def send(h, half, src, dst, ids):
        spots = pl.ds(pl.multiple_of(half * half_class, half_class), half_class)
        return remote(ctx.at[h, :, :, src, spots], ctx.at[h, :, :, dst, spots],
                      ctx_send.at[dst, h, half], ctx_recv.at[dst, h, half], ids)

    def send_own(h, half):
        return ((has_next, send(h, half, O, A, down)), (even, send(h, half, O, C, side)))

    def send_relay(h, half):
        return (((odd == 1) & (z > 0), send(h, half, A, C, side)),)

    def send_query(h):
        return ((z > 0, remote(q.at[h], visitor.at[h], q_sem.at[0, h], q_sem.at[1, h], up)),)

    def send_part(h):
        return ((has_next, remote(part.at[h], far_out.at[h], part_sem.at[0, h], part_sem.at[1, h], down)),
                (has_next, remote(part_lse.at[h], far_lse.at[h], lse_sem.at[0, h], lse_sem.at[1, h], down)))

    def start_all(sends):
        for condition, copy in sends:
            @pl.when(condition)
            def _():
                copy.start()

    def project_kv(h, half):
        if half is None:
            source, natural, span = x[...].reshape(rows, x.shape[2]), pl.ds(0, rows), (0, rows)
            spots = pl.ds(0, class_rows)
        else:
            source, natural = x[half], pl.ds(pl.multiple_of(half * half_rows, half_rows), half_rows)
            span, spots = (0, half_rows), pl.ds(pl.multiple_of(half * half_class, half_class), half_class)
        kv = jnp.dot(source, wkv[h], preferred_element_type=F32)
        k = rotated(kv[:, :HEAD], cos_ref[natural], sin_ref[natural])
        v = kv[:, HEAD:]
        flat_a[span[0]:span[1]] = k
        flat_b[span[0]:span[1]] = v
        kn[h, natural] = k.astype(BF16)
        vn[h, natural] = v.astype(BF16)
        count = span[1] // CLASSES
        for c in range(CLASSES):
            ctx[h, 0, c, O, spots] = flat_a[classed(0, count, c), :].astype(BF16)
            ctx[h, 1, c, O, spots] = flat_b[classed(0, count, c), :].astype(BF16)
        for part_half in (order if half is None else (half,)):
            start_all(send_own(h, part_half))

    kv_copy(0, 0).wait()
    kv_copy(0, 1).wait()
    project_kv(0, tp)
    lax.fori_loop(other * PIECES, other * PIECES + PIECES, table, 0)
    for i in range(PIECES):
        x_copy(i).wait_recv()
    project_kv(0, other)

    def project_rest(h, _):
        kv_copy(h, 0).wait()
        kv_copy(h, 1).wait()
        project_kv(h, None)
        return 0

    lax.fori_loop(1, heads, project_rest, 0)

    for copy in q_copies:
        copy.wait()

    def project_q(p, _):
        qq = jnp.dot(x[...].reshape(rows, x.shape[2]), wq[p], preferred_element_type=F32)
        for s, flat in ((0, flat_a), (1, flat_b)):
            r = rotated(qq[:, s * HEAD:(s + 1) * HEAD], cos_ref[...], sin_ref[...])
            flat[...] = r
            qn[2 * p + s] = r.astype(BF16)
            for c in range(CLASSES):
                q[2 * p + s, c] = flat[classed(0, class_rows, c), :].astype(BF16)
            start_all(send_query(2 * p + s))
        return 0

    lax.fori_loop(0, heads // 2, project_q, 0)

    def near(h, b, keys, vals, bias):
        scores = transposed_dot(qn[h, b * block:(b + 1) * block], keys) * SCALE + bias
        n, t, m = weighed(scores, vals)
        span = pl.ds(pl.multiple_of(h * rows, rows) + b * block, block)
        num[span, :] = n
        tot[span, :] = t
        top[span, :] = jnp.broadcast_to(m, (block, HEAD))

    def near_inner(h, _):
        for b in range(1, rows // block):
            span = slice((b - 1) * block, (b + 1) * block)
            near(h, b, kn[h, span], vn[h, span], band[1])
        return 0

    def poll(h, half):
        @pl.when((odd == 1) & (z > 0))
        def _():
            send(h, half, A, A, side).wait_recv()
        start_all(send_relay(h, half))

    poll(0, tp)
    lax.fori_loop(0, heads // 2, near_inner, 0)
    poll(0, other)
    lax.fori_loop(heads // 2, heads, near_inner, 0)

    def mix_copy(h):
        cols = pl.ds(pl.multiple_of((2 * h + tp) * HEAD, HEAD), HEAD)
        return remote(mixg.at[:, cols], mixg.at[:, cols], mix_send.at[h], mix_recv.at[h], across)

    eye = iota((block, block), 0) == iota((block, block), 1)

    def visit(h):
        @pl.when(has_next)
        def _():
            remote(q.at[h], visitor.at[h], q_sem.at[0, h], q_sem.at[1, h], side).wait_recv()
            for c in range(CLASSES):
                keys = ctx[h, 0, c, A:O].reshape(2 * class_rows, HEAD)
                vals = ctx[h, 1, c, A:O].reshape(2 * class_rows, HEAD)
                n, t, m = weighed(transposed_dot(visitor[h, c], keys) * SCALE + visit_bias[...], vals)
                part[h, c] = (n / t).astype(BF16)
                lse = m + jnp.log2(t)
                part_lse[h, c:c + 1, :] = jnp.sum(jnp.where(eye, lse, 0.0), axis=0, keepdims=True)

        start_all(send_part(h))

    def attend(h):
        tails = [jnp.concatenate([ctx[h, kind, c, C, class_rows - share:] for c in range(CLASSES)] + [nat[h, :block]], axis=0)
                 for kind, nat in ((0, kn), (1, vn))]
        near(h, 0, tails[0], tails[1], band[0])
        for c in range(CLASSES):
            keys = ctx[h, 0, c].reshape(SLOTS * class_rows, HEAD)
            vals = ctx[h, 1, c].reshape(SLOTS * class_rows, HEAD)
            n, t, m = weighed(transposed_dot(q[h, c], keys) * SCALE + far_bias[...], vals)
            span = classed(pl.multiple_of(h * rows, rows), class_rows, c)
            near_top = top[span, :]
            most = jnp.maximum(near_top, m)
            old, new = jnp.exp2(near_top - most), jnp.exp2(m - most)
            cnum[h, c] = num[span, :] * old + n * new
            ctot[h, c] = tot[span, :] * old + t * new
            ctop[h, c] = most

    def step(h, _):
        for half in order:
            @pl.when(even & (z > 0))
            def _():
                send(h, half, A, A, side).wait_recv()

            @pl.when(sp > 0)
            def _():
                send(h, half, C, C, side).wait_recv()
        visit(h)

        @pl.when(h + 1 < heads)
        def _():
            poll(h + 1, tp)
        attend(h)

        @pl.when(h + 1 < heads)
        def _():
            poll(h + 1, other)
        return 0

    lax.fori_loop(0, heads, step, 0)

    def combine(h, _):
        @pl.when(z > 0)
        def _():
            remote(part.at[h], far_out.at[h], part_sem.at[0, h], part_sem.at[1, h], side).wait_recv()
            remote(part_lse.at[h], far_lse.at[h], lse_sem.at[0, h], lse_sem.at[1, h], side).wait_recv()

        for c in range(CLASSES):
            lf = jnp.sum(jnp.where(eye, far_lse[h, c:c + 1, :], 0.0), axis=1, keepdims=True)
            ln = ctop[h, c]
            most = jnp.maximum(ln, lf)
            en, ef = jnp.exp2(ln - most), jnp.exp2(lf - most)
            mixed = (cnum[h, c] * en + far_out[h, c].astype(F32) * ef) / (ctot[h, c] * en + ef)
            mixf[classed(0, class_rows, c), :] = mixed
        cols = pl.ds(pl.multiple_of((2 * h + tp) * HEAD, HEAD), HEAD)
        mixg[:, cols] = mixf[...].astype(BF16)
        mix_copy(h).start()
        return 0

    def gathered(h, _):
        mix_copy(h).wait_recv()
        return 0

    lax.fori_loop(0, heads - 1, combine, 0)
    for copy in wo_copies:
        copy.wait()
    lax.fori_loop(0, heads - 1, gathered, 0)
    most_in = (heads - 1) * 2 * HEAD

    def partial_out(i, _):
        cols = pl.ds(pl.multiple_of(i * 256, 256), 256)
        out_sum[:, cols] = jnp.dot(mixg[:, :most_in], wo[:most_in, cols], preferred_element_type=F32)
        return 0

    lax.fori_loop(0, out_ref.shape[1] // 256, partial_out, 0)
    combine(heads - 1, 0)
    gathered(heads - 1, 0)

    def project_out(i, _):
        cols = pl.ds(pl.multiple_of(i * 256, 256), 256)
        last = jnp.dot(mixg[:, most_in:], wo[most_in:, cols], preferred_element_type=F32)
        out_ref[:, cols] = (out_sum[:, cols] + last).astype(BF16)
        return 0

    lax.fori_loop(0, out_ref.shape[1] // 256, project_out, 0)

    for i in range(PIECES):
        x_copy(i).wait_send()

    def left(h, _):
        sends = send_query(h) + send_part(h)
        for half in range(2):
            sends = sends + send_own(h, half) + send_relay(h, half)
        for condition, copy in sends:
            @pl.when(condition)
            def _():
                copy.wait_send()
        mix_copy(h).wait_send()
        return 0

    lax.fori_loop(0, heads, left, 0)


def body(tokens, query_weight, key_weight, value_weight, output_weight):
    n_sp = lax.axis_size("sp")
    half_rows, width = tokens.shape
    rows = half_rows * lax.axis_size("tp")
    heads = query_weight.shape[1] // HEAD
    assert rows * 4 == FAR_DILATION * REACH_STEPS and rows == 512
    assert n_sp % 2 == 0 and lax.axis_size("tp") == 2 and heads % 2 == 0 and heads >= 4

    half = HEAD // 2
    inverse = THETA_BASE ** (-np.arange(half, dtype=np.float64) / half)
    inverse = np.concatenate([inverse, inverse]).astype(np.float32)[None, :]

    class_rows = rows // CLASSES
    anywhere = pl.BlockSpec(memory_space=pl.ANY)
    vmem = pl.BlockSpec(memory_space=pltpu.VMEM)
    out_cols = output_weight.shape[1]
    dma = pltpu.SemaphoreType.DMA
    return pl.pallas_call(
        functools.partial(kernel, n_sp, heads),
        out_shape=pltpu.VMEM((rows, out_cols), BF16),
        in_specs=[anywhere] * 6,
        out_specs=vmem,
        scratch_shapes=[
            pltpu.VMEM((2, half_rows, width), BF16),
            pltpu.VMEM((heads, width, 2 * HEAD), BF16),
            pltpu.VMEM((heads // 2, width, 2 * HEAD), BF16),
            pltpu.VMEM(output_weight.shape, BF16),
            pltpu.VMEM((1, HEAD), F32),
            pltpu.VMEM((rows, HEAD), F32),
            pltpu.VMEM((rows, HEAD), F32),
            pltpu.VMEM((heads, 2, CLASSES, SLOTS, class_rows, HEAD), BF16),
            pltpu.VMEM((heads, CLASSES, class_rows, HEAD), BF16),
            pltpu.VMEM((heads, rows, HEAD), BF16),
            pltpu.VMEM((heads, rows, HEAD), BF16),
            pltpu.VMEM((heads, rows, HEAD), BF16),
            pltpu.VMEM((heads, CLASSES, class_rows, HEAD), BF16),
            pltpu.VMEM((rows, HEAD), F32),
            pltpu.VMEM((rows, HEAD), F32),
            pltpu.VMEM((REACH_STEPS, SLOTS * REACH_STEPS), F32),
            pltpu.VMEM((REACH_STEPS, 2 * REACH_STEPS), F32),
            pltpu.VMEM((2, REACH_STEPS, 2 * REACH_STEPS), F32),
            pltpu.VMEM((heads * rows, HEAD), F32),
            pltpu.VMEM((heads * rows, HEAD), F32),
            pltpu.VMEM((heads * rows, HEAD), F32),
            pltpu.VMEM((heads, CLASSES, class_rows, HEAD), F32),
            pltpu.VMEM((heads, CLASSES, class_rows, HEAD), F32),
            pltpu.VMEM((heads, CLASSES, class_rows, HEAD), F32),
            pltpu.VMEM((heads, CLASSES, class_rows, HEAD), BF16),
            pltpu.VMEM((heads, 8, 128), F32),
            pltpu.VMEM((heads, CLASSES, class_rows, HEAD), BF16),
            pltpu.VMEM((heads, 8, 128), F32),
            pltpu.VMEM((rows, HEAD), F32),
            pltpu.VMEM((rows, 2 * heads * HEAD), BF16),
            pltpu.VMEM((rows, out_cols), F32),
            dma((PIECES,)),
            dma((2, heads)),
            dma((heads // 2,)),
            dma((2, heads)),
            dma((1,)),
            dma((PIECES,)),
            dma((PIECES,)),
            dma((2, heads, 2)),
            dma((2, heads, 2)),
            dma((2, heads)),
            dma((2, heads)),
            dma((2, heads)),
            dma((heads,)),
            dma((heads,)),
        ],
        compiler_params=pltpu.CompilerParams(
            collective_id=0, has_side_effects=True, vmem_limit_bytes=56 * 1024 * 1024
        ),
    )(tokens, query_weight, key_weight, value_weight, output_weight, jnp.asarray(inverse))


def solution(mesh):
    in_specs = (
        P(("grp", "sp", "tp"), None),
        P(None, "tp"),
        P(None, "tp"),
        P(None, "tp"),
        P(None, "tp"),
    )
    out_specs = P(("grp", "sp"), "tp")
    return jax.shard_map(body, mesh=mesh, in_specs=in_specs, out_specs=out_specs, check_vma=False)
```

```python
import functools

import jax
import jax.numpy as jnp
import numpy as np
from jax import lax
from jax.experimental import pallas as pl
from jax.experimental.pallas import tpu as pltpu
from jax.sharding import PartitionSpec as P

HEAD = 128
REACH_STEPS = 128
MIDDLE_DILATION = 4
FAR_DILATION = 16
THETA_BASE = 500000.0
NEG = -1e30
MESH = pl.DeviceIdType.MESH
F32 = jnp.float32
BF16 = jnp.bfloat16
SCALE = HEAD ** -0.5 / float(np.log(2.0))

A, C, O = 0, 1, 2
SLOTS = 3
CLASSES = MIDDLE_DILATION
PIECES = 2


def iota(shape, dim):
    return lax.broadcasted_iota(jnp.int32, shape, dim)


def rotated(x, cosine, sine):
    return x * cosine + pltpu.roll(x, HEAD // 2, 1) * sine


def weighed(scores, values):
    top = jnp.max(scores, axis=-1, keepdims=True)
    raised = jnp.exp2(scores - top).astype(BF16)
    ones = jnp.ones(values.shape, BF16)
    both = jnp.dot(raised, jnp.concatenate([values, ones], axis=1), preferred_element_type=F32)
    return both[:, :HEAD], both[:, HEAD:], top


def transposed_dot(a, b):
    return lax.dot_general(a, b, (((1,), (1,)), ((), ())), preferred_element_type=F32)


def classed(start, count, c):
    return pl.ds(start + c, count, stride=CLASSES)


def kernel(
    n_sp, heads, guests,
    tok_hbm, wq_hbm, wk_hbm, wv_hbm, wo_hbm, inv_hbm,
    out_ref,
    x, wkv, wq, wo, inv, cos_ref, sin_ref, ctx, q, qn, kn, vn, visitor, second, flat_a, flat_b,
    far_bias, visit_bias, pair_bias, band, num, tot, top, cnum, ctot, ctop, vnum, vtot, vtop,
    part, part_lse, far_out, far_lse, back, back_lse, mid_out, mid_lse, mixf, mixg, out_sum,
    tok_sem, kv_sem, q_load, wo_sem, inv_sem, x_send, x_recv,
    ctx_send, ctx_recv, q_sem, second_sem, part_sem, lse_sem, mid_sem, mid_lse_sem, mix_send, mix_recv,
):
    sp = lax.axis_index("sp")
    tp = lax.axis_index("tp")
    z = sp // 2
    odd = sp % 2
    even = odd == 0
    other = 1 - tp
    has_next = z + 1 < n_sp // 2
    has_second = z + 2 < n_sp // 2
    half_rows = x.shape[1]
    rows = 2 * half_rows
    class_rows = rows // CLASSES
    half_class = class_rows // 2
    piece = half_rows // PIECES
    order = (tp, other)

    tok_copies = []
    for i in range(PIECES):
        span = pl.ds(i * piece, piece)
        copy = pltpu.make_async_copy(tok_hbm.at[span], x.at[tp, span], tok_sem.at[i])
        copy.start()
        tok_copies.append(copy)
    inv_copy = pltpu.make_async_copy(inv_hbm, inv, inv_sem.at[0])
    inv_copy.start()

    def kv_copy(h, kind):
        source = (wk_hbm, wv_hbm)[kind]
        cols = pl.ds(h * HEAD, HEAD)
        return pltpu.make_async_copy(source.at[:, cols], wkv.at[h, :, pl.ds(kind * HEAD, HEAD)], kv_sem.at[kind, h])

    q_copies = [
        pltpu.make_async_copy(wq_hbm.at[:, pl.ds(p * 2 * HEAD, 2 * HEAD)], wq.at[p], q_load.at[p])
        for p in range(heads // 2)]
    q_copies[0].start()
    for h in (guests, 0):
        for kind in range(2):
            kv_copy(h, kind).start()
    wo_copies = [
        pltpu.make_async_copy(
            wo_hbm.at[pl.ds((t * heads + h) * HEAD, HEAD)], wo.at[pl.ds((2 * h + t) * HEAD, HEAD)], wo_sem.at[t, h])
        for h in range(heads) for t in range(2)]

    barrier = pltpu.get_barrier_semaphore()
    y_partner = sp + 1 - 2 * odd

    def greet(ids):
        pl.semaphore_signal(barrier, inc=1, device_id=ids, device_id_type=MESH)

    greet({"tp": other})
    greet({"sp": y_partner})

    @pl.when(has_next)
    def _():
        greet({"sp": sp + 2})

    @pl.when(z > 0)
    def _():
        greet({"sp": sp - 2})

    def remote(src, dst, send_sem, recv_sem, ids):
        return pltpu.make_async_remote_copy(
            src_ref=src, dst_ref=dst, send_sem=send_sem, recv_sem=recv_sem,
            device_id=ids, device_id_type=MESH)

    down = {"sp": sp + 2}
    up = {"sp": sp - 2}
    side = {"sp": y_partner}
    across = {"tp": other}

    block = REACH_STEPS
    share = block // CLASSES
    ratio = FAR_DILATION // MIDDLE_DILATION

    def masks():
        qi, kj = iota((block, SLOTS * block), 0), iota((block, SLOTS * block), 1)
        slot = kj // block
        apart = qi - (kj % block)

        def bias(dist, here):
            steps = apart + block * dist
            mid = here & (steps >= 0) & (steps <= REACH_STEPS)
            far = here & (steps >= 0) & (steps % ratio == 0) & (steps <= ratio * REACH_STEPS)
            return jnp.where(mid & far, 1.0, jnp.where(mid | far, 0.0, NEG))

        far_bias[...] = bias(O - slot, O - slot <= sp)
        visit_bias[...] = bias(O + 2 - slot, O - slot <= sp)[:, :O * block]
        pair_bias[0] = bias(O - slot, (slot == O) | (odd == 1))[:, C * block:]
        pair_bias[1] = bias(jnp.where(slot == O, 2, 1 + 2 * odd), slot >= C)[:, C * block:]
        pair_bias[2] = bias(jnp.where(slot == O, 4, 3 + 2 * odd), slot >= C)[:, C * block:]
        ni, nj = iota((block, 2 * block), 0), iota((block, 2 * block), 1)
        gap = ni + block - nj
        band[1] = jnp.where((gap >= 0) & (gap <= REACH_STEPS), 0.0, NEG)
        gap = jnp.where(nj < block, ni + block - ((nj % share) * CLASSES + nj // share), gap)
        near_ok = (gap >= 0) & (gap <= REACH_STEPS)
        band[0] = jnp.where(near_ok & ((nj >= block) | (sp > 0)), 0.0, NEG)
        band[2] = jnp.where(near_ok & ((nj >= block) | (odd == 1)), 0.0, NEG)
        gap = ((ni % share) - (nj % share)) * CLASSES + ni // share - nj // share + block
        band[3] = jnp.where((gap >= 0) & (gap <= REACH_STEPS) & even & (nj < block), 0.0, NEG)

        for slot_at in (A, C):
            @pl.when(sp < 2 - slot_at)
            def _():
                def clear(h, _):
                    ctx[h, :, :, slot_at] = jnp.zeros((2, CLASSES, class_rows, HEAD), BF16)
                    return 0
                lax.fori_loop(guests, heads, clear, 0)

        part_lse[...] = jnp.zeros(part_lse.shape, F32)
        back_lse[...] = jnp.zeros(back_lse.shape, F32)

        @pl.when(z == 0)
        def _():
            far_out[...] = jnp.zeros(far_out.shape, BF16)
            far_lse[...] = jnp.full(far_lse.shape, NEG, F32)
            mid_out[...] = jnp.zeros(mid_out.shape, BF16)
            mid_lse[...] = jnp.full(mid_lse.shape, NEG, F32)

    lane = iota((piece, HEAD), 1)

    def table(c, _):
        start = pl.multiple_of(c * piece, piece)
        positions = sp * rows + start + iota((piece, HEAD), 0)
        angles = positions.astype(F32) * inv[...]
        span = pl.ds(start, piece)
        cos_ref[span, :] = jnp.cos(angles)
        sine = jnp.sin(angles)
        sin_ref[span, :] = jnp.where(lane < HEAD // 2, -sine, sine)
        return 0

    inv_copy.wait()
    lax.fori_loop(tp * PIECES, tp * PIECES + PIECES, table, 0)

    pl.semaphore_wait(barrier, 2 + has_next.astype(jnp.int32) + (z > 0).astype(jnp.int32))

    def x_copy(i):
        span = pl.ds(i * piece, piece)
        return remote(x.at[tp, span], x.at[tp, span], x_send.at[i], x_recv.at[i], across)

    for i in range(PIECES):
        tok_copies[i].wait()
        x_copy(i).start()
    for h in (*range(1, guests), *range(guests + 1, heads)):
        for kind in range(2):
            kv_copy(h, kind).start()
    for copy in (*q_copies[1:], *wo_copies):
        copy.start()

    def send(h, half, src, dst, ids):
        spots = pl.ds(pl.multiple_of(half * half_class, half_class), half_class)
        return remote(ctx.at[h, :, :, src, spots], ctx.at[h, :, :, dst, spots],
                      ctx_send.at[dst, h, half], ctx_recv.at[dst, h, half], ids)

    def send_down(h, half):
        return () if h < guests else ((has_next, send(h, half, O, A, down)),)

    def send_side(h, half):
        return ((even | (h < guests), send(h, half, O, C, side)),)

    def send_relay(h, half):
        return () if h < guests else (((odd == 1) & (z > 0), send(h, half, A, C, side)),)

    def query_copy(h, half):
        spots = pl.ds(pl.multiple_of(half * half_class, half_class), half_class)
        return remote(q.at[h, :, spots], visitor.at[h, :, spots], q_sem.at[0, h, half], q_sem.at[1, h, half], up)

    def send_query(h, half):
        return ((z > 0, query_copy(h, half)),)

    def second_copy(h):
        return remote(visitor.at[h], second.at[h], second_sem.at[0, h], second_sem.at[1, h], up)

    def send_second(h):
        return ((has_next & (z > 0), second_copy(h)),) if h < guests else ()

    def back_copies(h):
        return (remote(back.at[h], mid_out.at[h], mid_sem.at[0, h], mid_sem.at[1, h], down),
                remote(back_lse.at[h], mid_lse.at[h], mid_lse_sem.at[0, h], mid_lse_sem.at[1, h], down))

    def send_back(h):
        return tuple((has_second, copy) for copy in back_copies(h)) if h < guests else ()

    def send_part(h):
        return ((has_next, remote(part.at[h], far_out.at[h], part_sem.at[0, h], part_sem.at[1, h], down)),
                (has_next, remote(part_lse.at[h], far_lse.at[h], lse_sem.at[0, h], lse_sem.at[1, h], down)))

    def start_all(sends):
        for condition, copy in sends:
            @pl.when(condition)
            def _():
                copy.start()

    def project_kv(h, half):
        if half is None:
            source, natural, span = x[...].reshape(rows, x.shape[2]), pl.ds(0, rows), (0, rows)
            spots = pl.ds(0, class_rows)
        else:
            source, natural = x[half], pl.ds(pl.multiple_of(half * half_rows, half_rows), half_rows)
            span, spots = (0, half_rows), pl.ds(pl.multiple_of(half * half_class, half_class), half_class)
        kv = jnp.dot(source, wkv[h], preferred_element_type=F32)
        k = rotated(kv[:, :HEAD], cos_ref[natural], sin_ref[natural])
        v = kv[:, HEAD:]
        flat_a[span[0]:span[1]] = k
        flat_b[span[0]:span[1]] = v
        kn[h, natural] = k.astype(BF16)
        vn[h, natural] = v.astype(BF16)
        count = span[1] // CLASSES
        for c in range(CLASSES):
            ctx[h, 0, c, O, spots] = flat_a[classed(0, count, c), :].astype(BF16)
            ctx[h, 1, c, O, spots] = flat_b[classed(0, count, c), :].astype(BF16)
        for part_half in (order if half is None else (half,)):
            start_all(send_down(h, part_half))
            if h < guests:
                start_all(send_side(h, part_half))

    def project_q(p, half):
        if half is None:
            source, natural, count = x[...].reshape(rows, x.shape[2]), pl.ds(0, rows), rows
            spots = pl.ds(0, class_rows)
        else:
            source, natural = x[half], pl.ds(pl.multiple_of(half * half_rows, half_rows), half_rows)
            count, spots = half_rows, pl.ds(pl.multiple_of(half * half_class, half_class), half_class)
        qq = jnp.dot(source, wq[p], preferred_element_type=F32)
        for s, flat in ((0, flat_a), (1, flat_b)):
            r = rotated(qq[:, s * HEAD:(s + 1) * HEAD], cos_ref[natural], sin_ref[natural])
            flat[0:count] = r
            qn[2 * p + s, natural] = r.astype(BF16)
            for c in range(CLASSES):
                q[2 * p + s, c, spots] = flat[classed(0, count // CLASSES, c), :].astype(BF16)
            if half is not None:
                start_all(send_query(2 * p + s, half))

    def load_kv(h):
        kv_copy(h, 0).wait()
        kv_copy(h, 1).wait()

    def near(h, b, keys, vals, bias):
        scores = transposed_dot(qn[h, b * block:(b + 1) * block], keys) * SCALE + bias
        n, t, m = weighed(scores, vals)
        span = pl.ds(pl.multiple_of(h * rows, rows) + b * block, block)
        num[span, :] = n
        tot[span, :] = t
        top[span, :] = jnp.broadcast_to(m, (block, HEAD))

    def near_inner(h, _):
        for b in range(1, rows // block):
            span = slice((b - 1) * block, (b + 1) * block)
            near(h, b, kn[h, span], vn[h, span], band[1])
        return 0

    def load_kv(h):
        kv_copy(h, 0).wait()
        kv_copy(h, 1).wait()

    def poll(h):
        for half in order:
            @pl.when((odd == 1) & (z > 0))
            def _():
                send(h, half, A, A, side).wait_recv()
            start_all(send_relay(h, half))

    def meet(h):
        @pl.when(has_next)
        def _():
            for half in order:
                query_copy(h, half).wait_recv()
        start_all(send_second(h))

    def neighbours(h):
        for half in order:
            if h >= guests:
                @pl.when(even & (z > 0))
                def _():
                    send(h, half, A, A, side).wait_recv()

                @pl.when(sp > 0)
                def _():
                    send(h, half, C, C, side).wait_recv()
            else:
                send(h, half, C, C, side).wait_recv()

    def mix_copy(h):
        cols = pl.ds(pl.multiple_of((2 * h + tp) * HEAD, HEAD), HEAD)
        return remote(mixg.at[:, cols], mixg.at[:, cols], mix_send.at[h], mix_recv.at[h], across)

    eye = iota((block, block), 0) == iota((block, block), 1)

    def context(h, c, kind, first, last):
        return ctx[h, kind, c, first:last].reshape((last - first) * class_rows, HEAD)

    def visit(h, guest, bias, first, last, result, lse):
        for c in range(CLASSES):
            keys, vals = (context(h, c, kind, first, last) for kind in range(2))
            n, t, m = weighed(transposed_dot(guest[h, c], keys) * SCALE + bias, vals)
            result[h, c] = (n / t).astype(BF16)
            lse[h, c:c + 1, :] = jnp.sum(jnp.where(eye, m + jnp.log2(t), 0.0), axis=0, keepdims=True)

    def visit_far(h):
        meet(h)

        @pl.when(has_next)
        def _():
            visit(h, visitor, visit_bias[...], A, O, part, part_lse)
        start_all(send_part(h))

    def visit_second(h):
        @pl.when(has_second)
        def _():
            second_copy(h).wait_recv()
            visit(h, second, pair_bias[2], C, SLOTS, back, back_lse)
        start_all(send_back(h))

    def tail_of(h, kind):
        return [ctx[h, kind, c, C, class_rows - share:] for c in range(CLASSES)]

    def join(n, t, m, n2, t2, m2):
        most = jnp.maximum(m, m2)
        old, new = jnp.exp2(m - most), jnp.exp2(m2 - most)
        return n * old + n2 * new, t * old + t2 * new, most

    def visit_first(h):
        @pl.when(has_next)
        def _():
            keys, vals = (jnp.concatenate(tail_of(h, kind), axis=0) for kind in range(2))
            guest = jnp.concatenate([visitor[h, c, :share] for c in range(CLASSES)], axis=0)
            close = weighed(transposed_dot(guest, keys) * SCALE + band[3, :, :block], vals)
            for c in range(CLASSES):
                keys, vals = (context(h, c, kind, C, SLOTS) for kind in range(2))
                n, t, m = weighed(transposed_dot(visitor[h, c], keys) * SCALE + pair_bias[1], vals)
                m = jnp.broadcast_to(m, (block, HEAD))
                vnum[h, c], vtot[h, c], vtop[h, c] = n, t, m
                n, t, m = join(n[:share], t[:share], m[:share], *(v[c * share:(c + 1) * share] for v in close))
                vnum[h, c, :share], vtot[h, c, :share], vtop[h, c, :share] = n, t, m

    def with_far(n, t, m, result, lse_row):
        lf = jnp.sum(jnp.where(eye, lse_row, 0.0), axis=1, keepdims=True)
        most = jnp.maximum(m, lf)
        en, ef = jnp.exp2(m - most), jnp.exp2(lf - most)
        total = t * en + ef
        return (n * en + result.astype(F32) * ef) / total, total, most

    def merge(h):
        @pl.when(has_next)
        def _():
            @pl.when(z > 0)
            def _():
                for copy in back_copies(h):
                    copy.wait_recv()
            for c in range(CLASSES):
                r, t, m = with_far(vnum[h, c], vtot[h, c], vtop[h, c], mid_out[h, c], mid_lse[h, c:c + 1, :])
                part[h, c] = r.astype(BF16)
                part_lse[h, c:c + 1, :] = jnp.sum(jnp.where(eye, m + jnp.log2(t), 0.0), axis=0, keepdims=True)
        start_all(send_part(h))

    def attend(h):
        first, bias, close = (C, pair_bias[0], band[2]) if h < guests else (A, far_bias[...], band[0])
        keys, vals = (jnp.concatenate(tail_of(h, kind) + [nat[h, :block]], axis=0)
                      for kind, nat in ((0, kn), (1, vn)))
        near(h, 0, keys, vals, close)
        for c in range(CLASSES):
            keys, vals = (context(h, c, kind, first, SLOTS) for kind in range(2))
            n, t, m = weighed(transposed_dot(q[h, c], keys) * SCALE + bias, vals)
            span = classed(h * rows, class_rows, c)
            cnum[h, c], ctot[h, c], ctop[h, c] = join(num[span, :], tot[span, :], top[span, :], n, t, m)

    def combine(h, _):
        @pl.when(z > 0)
        def _():
            remote(part.at[h], far_out.at[h], part_sem.at[0, h], part_sem.at[1, h], side).wait_recv()
            remote(part_lse.at[h], far_lse.at[h], lse_sem.at[0, h], lse_sem.at[1, h], side).wait_recv()

        for c in range(CLASSES):
            mixed, _, _ = with_far(cnum[h, c], ctot[h, c], ctop[h, c], far_out[h, c], far_lse[h, pl.ds(c, 1), :])
            mixf[classed(0, class_rows, c), :] = mixed
        cols = pl.ds(pl.multiple_of((2 * h + tp) * HEAD, HEAD), HEAD)
        mixg[:, cols] = mixf[...].astype(BF16)
        mix_copy(h).start()
        return 0

    def gathered(h, _):
        mix_copy(h).wait_recv()
        return 0

    out_cols = out_ref.shape[1]
    wide = 256

    def add_last(t, into):
        span = pl.ds(pl.multiple_of((2 * (heads - 1) + t) * HEAD, HEAD), HEAD)
        for i in range(out_cols // wide):
            cols = pl.ds(i * wide, wide)
            total = jnp.dot(mixg[:, span], wo[span, cols], preferred_element_type=F32)
            into[:, cols] = (out_sum[:, cols] + total).astype(into.dtype)

    def partial_out():
        most_in = (heads - 1) * 2 * HEAD
        for i in range(out_cols // wide):
            cols = pl.ds(i * wide, wide)
            out_sum[:, cols] = jnp.dot(mixg[:, :most_in], wo[:most_in, cols], preferred_element_type=F32)

    q_copies[0].wait()
    project_q(0, tp)
    load_kv(guests)
    project_kv(guests, tp)
    load_kv(0)
    project_kv(0, tp)
    lax.fori_loop(other * PIECES, other * PIECES + PIECES, table, 0)
    for i in range(PIECES):
        x_copy(i).wait_recv()
    project_q(0, other)
    project_kv(guests, other)
    project_kv(0, other)
    for h in (*range(1, guests), *range(guests + 1, heads)):
        load_kv(h)
        project_kv(h, None)
    for h in range(guests, heads):
        for half in order:
            start_all(send_side(h, half))
    meet(0)
    for p in range(1, heads // 2):
        q_copies[p].wait()
        project_q(p, None)
    masks()
    for h in range(1, guests):
        meet(h)
    for h in range(2, heads):
        for half in order:
            start_all(send_query(h, half))
    lax.fori_loop(0, heads // 2, near_inner, 0)
    poll(guests)
    lax.fori_loop(heads // 2, heads, near_inner, 0)
    neighbours(0)
    visit_first(0)
    attend(0)
    visit_second(0)
    for h in range(1, guests):
        poll(guests + h)
        neighbours(h)
        visit_second(h)
        visit_first(h)
        attend(h)
    for h in range(2 * guests, heads):
        poll(h)
    for h in range(guests):
        merge(h)
    for h in range(guests, heads):
        neighbours(h)
        visit_far(h)
        attend(h)
        if h < heads - 1:
            combine(h - guests, 0)
    for h in range(heads - guests - 1, heads - 1):
        combine(h, 0)
    for copy in wo_copies:
        copy.wait()
    for h in range(heads - 1):
        gathered(h, 0)
    partial_out()
    combine(heads - 1, 0)
    add_last(tp, out_sum)
    gathered(heads - 1, 0)
    add_last(other, out_ref)

    for i in range(PIECES):
        x_copy(i).wait_send()

    for h in range(heads):
        sends = send_second(h) + send_back(h) + send_part(h)
        for half in range(2):
            sends = sends + send_down(h, half) + send_side(h, half) + send_relay(h, half) + send_query(h, half)
        for condition, copy in sends:
            @pl.when(condition)
            def _():
                copy.wait_send()
        mix_copy(h).wait_send()


def body(tokens, query_weight, key_weight, value_weight, output_weight):
    n_sp = lax.axis_size("sp")
    half_rows, width = tokens.shape
    rows = half_rows * lax.axis_size("tp")
    heads = query_weight.shape[1] // HEAD
    assert rows * 4 == FAR_DILATION * REACH_STEPS and rows == 512
    assert n_sp % 2 == 0 and lax.axis_size("tp") == 2 and heads % 2 == 0 and heads >= 4

    half = HEAD // 2
    inverse = THETA_BASE ** (-np.arange(half, dtype=np.float64) / half)
    inverse = np.concatenate([inverse, inverse]).astype(np.float32)[None, :]

    guests = heads // 2
    class_rows = rows // CLASSES
    anywhere = pl.BlockSpec(memory_space=pl.ANY)
    vmem = pl.BlockSpec(memory_space=pltpu.VMEM)
    out_cols = output_weight.shape[1]
    dma = pltpu.SemaphoreType.DMA
    return pl.pallas_call(
        functools.partial(kernel, n_sp, heads, guests),
        out_shape=pltpu.VMEM((rows, out_cols), BF16),
        in_specs=[anywhere] * 6,
        out_specs=vmem,
        scratch_shapes=[
            pltpu.VMEM((2, half_rows, width), BF16),
            pltpu.VMEM((heads, width, 2 * HEAD), BF16),
            pltpu.VMEM((heads // 2, width, 2 * HEAD), BF16),
            pltpu.VMEM(output_weight.shape, BF16),
            pltpu.VMEM((1, HEAD), F32),
            pltpu.VMEM((rows, HEAD), F32),
            pltpu.VMEM((rows, HEAD), F32),
            pltpu.VMEM((heads, 2, CLASSES, SLOTS, class_rows, HEAD), BF16),
            pltpu.VMEM((heads, CLASSES, class_rows, HEAD), BF16),
            pltpu.VMEM((heads, rows, HEAD), BF16),
            pltpu.VMEM((heads, rows, HEAD), BF16),
            pltpu.VMEM((heads, rows, HEAD), BF16),
            pltpu.VMEM((heads, CLASSES, class_rows, HEAD), BF16),
            pltpu.VMEM((guests, CLASSES, class_rows, HEAD), BF16),
            pltpu.VMEM((rows, HEAD), F32),
            pltpu.VMEM((rows, HEAD), F32),
            pltpu.VMEM((REACH_STEPS, SLOTS * REACH_STEPS), F32),
            pltpu.VMEM((REACH_STEPS, 2 * REACH_STEPS), F32),
            pltpu.VMEM((3, REACH_STEPS, 2 * REACH_STEPS), F32),
            pltpu.VMEM((4, REACH_STEPS, 2 * REACH_STEPS), F32),
            pltpu.VMEM((heads * rows, HEAD), F32),
            pltpu.VMEM((heads * rows, HEAD), F32),
            pltpu.VMEM((heads * rows, HEAD), F32),
            pltpu.VMEM((heads, CLASSES, class_rows, HEAD), F32),
            pltpu.VMEM((heads, CLASSES, class_rows, HEAD), F32),
            pltpu.VMEM((heads, CLASSES, class_rows, HEAD), F32),
            pltpu.VMEM((guests, CLASSES, class_rows, HEAD), F32),
            pltpu.VMEM((guests, CLASSES, class_rows, HEAD), F32),
            pltpu.VMEM((guests, CLASSES, class_rows, HEAD), F32),
            pltpu.VMEM((heads, CLASSES, class_rows, HEAD), BF16),
            pltpu.VMEM((heads, 8, 128), F32),
            pltpu.VMEM((heads, CLASSES, class_rows, HEAD), BF16),
            pltpu.VMEM((heads, 8, 128), F32),
            pltpu.VMEM((guests, CLASSES, class_rows, HEAD), BF16),
            pltpu.VMEM((guests, 8, 128), F32),
            pltpu.VMEM((guests, CLASSES, class_rows, HEAD), BF16),
            pltpu.VMEM((guests, 8, 128), F32),
            pltpu.VMEM((rows, HEAD), F32),
            pltpu.VMEM((rows, 2 * heads * HEAD), BF16),
            pltpu.VMEM((rows, out_cols), F32),
            dma((PIECES,)),
            dma((2, heads)),
            dma((heads // 2,)),
            dma((2, heads)),
            dma((1,)),
            dma((PIECES,)),
            dma((PIECES,)),
            dma((2, heads, 2)),
            dma((2, heads, 2)),
            dma((2, heads, 2)),
            dma((2, guests)),
            dma((2, heads)),
            dma((2, heads)),
            dma((2, guests)),
            dma((2, guests)),
            dma((heads,)),
            dma((heads,)),
        ],
        compiler_params=pltpu.CompilerParams(
            collective_id=0, has_side_effects=True, vmem_limit_bytes=56 * 1024 * 1024
        ),
    )(tokens, query_weight, key_weight, value_weight, output_weight, jnp.asarray(inverse))


def solution(mesh):
    in_specs = (
        P(("grp", "sp", "tp"), None),
        P(None, "tp"),
        P(None, "tp"),
        P(None, "tp"),
        P(None, "tp"),
    )
    out_specs = P(("grp", "sp"), "tp")
    return jax.shard_map(body, mesh=mesh, in_specs=in_specs, out_specs=out_specs, check_vma=False)
```

```python
import functools

import jax
import jax.numpy as jnp
import numpy as np
from jax import lax
from jax.experimental import pallas as pl
from jax.experimental.pallas import tpu as pltpu
from jax.sharding import PartitionSpec as P

HEAD = 128
REACH_STEPS = 128
MIDDLE_DILATION = 4
FAR_DILATION = 16
THETA_BASE = 500000.0
NEG = -1e30
MESH = pl.DeviceIdType.MESH
F32 = jnp.float32
BF16 = jnp.bfloat16
SCALE = HEAD ** -0.5 / float(np.log(2.0))

A, C, O = 0, 1, 2
SLOTS = 3
CLASSES = MIDDLE_DILATION
PIECES = 2


def iota(shape, dim):
    return lax.broadcasted_iota(jnp.int32, shape, dim)


def rotated(x, cosine, sine):
    return x * cosine + pltpu.roll(x, HEAD // 2, 1) * sine


def weighed(scores, values):
    top = jnp.max(scores, axis=-1, keepdims=True)
    raised = jnp.exp2(scores - top).astype(BF16)
    ones = jnp.ones(values.shape, BF16)
    both = jnp.dot(raised, jnp.concatenate([values, ones], axis=1), preferred_element_type=F32)
    return both[:, :HEAD], both[:, HEAD:], top


def transposed_dot(a, b):
    return lax.dot_general(a, b, (((1,), (1,)), ((), ())), preferred_element_type=F32)


def classed(start, count, c):
    return pl.ds(start + c, count, stride=CLASSES)


def kernel(
    n_sp, heads, guests,
    tok_hbm, wq_hbm, wk_hbm, wv_hbm, wo_hbm, inv_hbm,
    out_ref,
    x, wkv, wq, wo, inv, cos_ref, sin_ref, ctx, q, qn, kn, vn, visitor, second, flat_a, flat_b,
    far_bias, visit_bias, pair_bias, band, num, tot, top, cnum, ctot, ctop, vnum, vtot, vtop,
    part, part_lse, far_out, far_lse, back, back_lse, mid_out, mid_lse, mixf, mixg, out_sum,
    tok_sem, inv_sem, kv_sem, q_load, wo_sem, x_sem, sent,
    a_recv, c_recv, q_recv, second_recv, part_recv, lse_recv, mid_recv, mid_lse_recv, mix_recv,
):
    sp = lax.axis_index("sp")
    tp = lax.axis_index("tp")
    z = sp // 2
    odd = sp % 2
    even = odd == 0
    other = 1 - tp
    has_next = z + 1 < n_sp // 2
    has_second = z + 2 < n_sp // 2
    half_rows = x.shape[1]
    rows = 2 * half_rows
    class_rows = rows // CLASSES
    half_class = class_rows // 2
    piece = half_rows // PIECES
    order = (tp, other)

    inv_copy = pltpu.make_async_copy(inv_hbm, inv, inv_sem.at[0])
    inv_copy.start()
    tok_copy = pltpu.make_async_copy(tok_hbm, x.at[tp], tok_sem.at[0])
    tok_copy.start()

    def kv_copy(h, kind):
        source = (wk_hbm, wv_hbm)[kind]
        cols = pl.ds(h * HEAD, HEAD)
        return pltpu.make_async_copy(source.at[:, cols], wkv.at[h, :, pl.ds(kind * HEAD, HEAD)], kv_sem.at[h])

    q_copies = [
        pltpu.make_async_copy(wq_hbm.at[:, pl.ds(p * 2 * HEAD, 2 * HEAD)], wq.at[p], q_load.at[p])
        for p in range(heads // 2)]
    for kind in range(2):
        kv_copy(guests, kind).start()
    wo_copies = [
        pltpu.make_async_copy(
            wo_hbm.at[pl.ds((t * heads + h) * HEAD, HEAD)], wo.at[pl.ds((2 * h + t) * HEAD, HEAD)], wo_sem.at[0])
        for h in range(heads) for t in range(2)]

    barrier = pltpu.get_barrier_semaphore()
    y_partner = sp + 1 - 2 * odd

    def greet(ids):
        pl.semaphore_signal(barrier, inc=1, device_id=ids, device_id_type=MESH)

    greet({"tp": other})
    greet({"sp": y_partner})

    @pl.when(has_next)
    def _():
        greet({"sp": sp + 2})

    @pl.when(z > 0)
    def _():
        greet({"sp": sp - 2})

    def remote(src, dst, send_sem, recv_sem, ids):
        return pltpu.make_async_remote_copy(
            src_ref=src, dst_ref=dst, send_sem=send_sem, recv_sem=recv_sem,
            device_id=ids, device_id_type=MESH)

    down = {"sp": sp + 2}
    up = {"sp": sp - 2}
    side = {"sp": y_partner}
    across = {"tp": other}

    block = REACH_STEPS
    share = block // CLASSES
    ratio = FAR_DILATION // MIDDLE_DILATION

    def masks():
        qi, kj = iota((block, SLOTS * block), 0), iota((block, SLOTS * block), 1)
        slot = kj // block
        apart = qi - (kj % block)

        def bias(dist, here):
            steps = apart + block * dist
            mid = here & (steps >= 0) & (steps <= REACH_STEPS)
            far = here & (steps >= 0) & (steps % ratio == 0) & (steps <= ratio * REACH_STEPS)
            return jnp.where(mid & far, 1.0, jnp.where(mid | far, 0.0, NEG))

        far_bias[...] = bias(O - slot, O - slot <= sp)
        visit_bias[...] = bias(O + 2 - slot, O - slot <= sp)[:, :O * block]
        pair_bias[0] = bias(O - slot, (slot == O) | (odd == 1))[:, C * block:]
        pair_bias[1] = bias(jnp.where(slot == O, 2, 1 + 2 * odd), slot >= C)[:, C * block:]
        pair_bias[2] = bias(jnp.where(slot == O, 4, 3 + 2 * odd), slot >= C)[:, C * block:]
        ni, nj = iota((block, 2 * block), 0), iota((block, 2 * block), 1)
        gap = ni + block - nj
        band[1] = jnp.where((gap >= 0) & (gap <= REACH_STEPS), 0.0, NEG)
        gap = jnp.where(nj < block, ni + block - ((nj % share) * CLASSES + nj // share), gap)
        near_ok = (gap >= 0) & (gap <= REACH_STEPS)
        band[0] = jnp.where(near_ok & ((nj >= block) | (sp > 0)), 0.0, NEG)
        band[2] = jnp.where(near_ok & ((nj >= block) | (odd == 1)), 0.0, NEG)
        gap = ((ni % share) - (nj % share)) * CLASSES + ni // share - nj // share + block
        band[3] = jnp.where((gap >= 0) & (gap <= REACH_STEPS) & even & (nj < block), 0.0, NEG)

        for slot_at in (A, C):
            @pl.when(sp < 2 - slot_at)
            def _():
                def clear(h, _):
                    ctx[h, :, :, slot_at] = jnp.zeros((2, CLASSES, class_rows, HEAD), BF16)
                    return 0
                lax.fori_loop(guests, heads, clear, 0)

        part_lse[...] = jnp.zeros(part_lse.shape, F32)
        back_lse[...] = jnp.zeros(back_lse.shape, F32)

        @pl.when(z == 0)
        def _():
            far_out[...] = jnp.zeros(far_out.shape, BF16)
            far_lse[...] = jnp.full(far_lse.shape, NEG, F32)
            mid_out[...] = jnp.zeros(mid_out.shape, BF16)
            mid_lse[...] = jnp.full(mid_lse.shape, NEG, F32)

    lane = iota((piece, HEAD), 1)

    def table(c, _):
        start = pl.multiple_of(c * piece, piece)
        positions = sp * rows + start + iota((piece, HEAD), 0)
        angles = positions.astype(F32) * inv[...]
        span = pl.ds(start, piece)
        cos_ref[span, :] = jnp.cos(angles)
        sine = jnp.sin(angles)
        sin_ref[span, :] = jnp.where(lane < HEAD // 2, -sine, sine)
        return 0

    inv_copy.wait()
    for kind in range(2):
        kv_copy(0, kind).start()
    q_copies[0].start()
    lax.fori_loop(tp * PIECES, tp * PIECES + PIECES, table, 0)

    pl.semaphore_wait(barrier, 2 + has_next.astype(jnp.int32) + (z > 0).astype(jnp.int32))

    x_copy = remote(x.at[tp], x.at[tp], x_sem.at[0], x_sem.at[1], across)
    tok_copy.wait()
    x_copy.start()
    for h in (*range(guests + 1, heads), *range(1, guests)):
        for kind in range(2):
            kv_copy(h, kind).start()
    for copy in (*q_copies[1:], *wo_copies):
        copy.start()

    DOWN, SIDE, RELAY, ASK, SECOND, PART, LSE, MID, MID_LSE, MIX = range(10)

    def spots_of(half):
        return pl.ds(pl.multiple_of(half * half_class, half_class), half_class)

    def block_copy(h, src, dst, rows_at, kind, ids):
        arrived = a_recv.at[h - guests] if dst == A else c_recv.at[h]
        return remote(ctx.at[h, :, :, src, rows_at], ctx.at[h, :, :, dst, rows_at], sent.at[kind], arrived, ids)

    every = pl.ds(0, class_rows)

    def send_down(h, half):
        return ((has_next & (h >= guests), block_copy(jnp.maximum(h, guests), O, A, spots_of(half), DOWN, down)),)

    def send_side(h, half):
        return ((even | (h < guests), block_copy(h, O, C, spots_of(half), SIDE, side)),)

    def send_relay(h):
        return (((odd == 1) & (z > 0), block_copy(h, A, C, every, RELAY, side)),)

    def query_copy(h, half):
        rows_at, arrived = (spots_of(half), q_recv.at[2 * h + half]) if h < guests else (every, q_recv.at[guests + h])
        return remote(q.at[h, :, rows_at], visitor.at[h, :, rows_at], sent.at[ASK], arrived, up)

    def second_copy(h, rows_at):
        return remote(visitor.at[h, :, rows_at], second.at[h, :, rows_at], sent.at[SECOND], second_recv.at[h], up)

    def back_copies(h):
        return (remote(back.at[h], mid_out.at[h], sent.at[MID], mid_recv.at[h], down),
                remote(back_lse.at[h], mid_lse.at[h], sent.at[MID_LSE], mid_lse_recv.at[h], down))

    def part_copies(h):
        return (remote(part.at[h], far_out.at[h], sent.at[PART], part_recv.at[h], down),
                remote(part_lse.at[h], far_lse.at[h], sent.at[LSE], lse_recv.at[h], down))

    def send_back(h):
        return tuple((has_second, copy) for copy in back_copies(h))

    def send_part(h):
        return tuple((has_next, copy) for copy in part_copies(h))

    def start_all(sends):
        for condition, copy in sends:
            @pl.when(condition)
            def _():
                copy.start()

    def project_kv(h, half):
        if half is None:
            source, natural, span = x[...].reshape(rows, x.shape[2]), pl.ds(0, rows), (0, rows)
            spots = pl.ds(0, class_rows)
        else:
            source, natural = x[half], pl.ds(pl.multiple_of(half * half_rows, half_rows), half_rows)
            span, spots = (0, half_rows), pl.ds(pl.multiple_of(half * half_class, half_class), half_class)
        kv = jnp.dot(source, wkv[h], preferred_element_type=F32)
        k = rotated(kv[:, :HEAD], cos_ref[natural], sin_ref[natural])
        v = kv[:, HEAD:]
        flat_a[span[0]:span[1]] = k
        flat_b[span[0]:span[1]] = v
        kn[h, natural] = k.astype(BF16)
        vn[h, natural] = v.astype(BF16)
        count = span[1] // CLASSES
        for c in range(CLASSES):
            ctx[h, 0, c, O, spots] = flat_a[classed(0, count, c), :].astype(BF16)
            ctx[h, 1, c, O, spots] = flat_b[classed(0, count, c), :].astype(BF16)
        for part_half in (order if half is None else (half,)):
            start_all(send_down(h, part_half))
            for condition, copy in send_side(h, part_half):
                @pl.when(h < guests)
                def _():
                    copy.start()

    def project_q(p, half):
        if half is None:
            source, natural, count = x[...].reshape(rows, x.shape[2]), pl.ds(0, rows), rows
            spots = pl.ds(0, class_rows)
        else:
            source, natural = x[half], pl.ds(pl.multiple_of(half * half_rows, half_rows), half_rows)
            count, spots = half_rows, pl.ds(pl.multiple_of(half * half_class, half_class), half_class)
        qq = jnp.dot(source, wq[p], preferred_element_type=F32)
        for s, flat in ((0, flat_a), (1, flat_b)):
            r = rotated(qq[:, s * HEAD:(s + 1) * HEAD], cos_ref[natural], sin_ref[natural])
            flat[0:count] = r
            qn[2 * p + s, natural] = r.astype(BF16)
            for c in range(CLASSES):
                q[2 * p + s, c, spots] = flat[classed(0, count // CLASSES, c), :].astype(BF16)

    def near(h, b, keys, vals, bias):
        scores = transposed_dot(qn[h, b * block:(b + 1) * block], keys) * SCALE + bias
        n, t, m = weighed(scores, vals)
        span = pl.ds(pl.multiple_of(h * rows, rows) + b * block, block)
        num[span, :] = n
        tot[span, :] = t
        top[span, :] = jnp.broadcast_to(m, (block, HEAD))

    def near_inner(h):
        for b in range(1, rows // block):
            span = slice((b - 1) * block, (b + 1) * block)
            near(h, b, kn[h, span], vn[h, span], band[1])

    def load_kv(h):
        pltpu.make_async_copy(wk_hbm.at[:, pl.ds(0, 2 * HEAD)], wkv.at[h], kv_sem.at[h]).wait()

    def poll(h):
        @pl.when((odd == 1) & (z > 0))
        def _():
            block_copy(h, A, A, every, RELAY, side).wait_recv()
        start_all(send_relay(h))

    def meet(h, half):
        @pl.when(has_next)
        def _():
            query_copy(h, half).wait_recv()
        if h < guests:
            @pl.when(has_next & (z > 0))
            def _():
                second_copy(h, spots_of(half)).start()

    def neighbours(h):
        if h < guests:
            block_copy(h, C, C, every, SIDE, side).wait_recv()
        else:
            @pl.when(even & (z > 0))
            def _():
                block_copy(h, A, A, every, RELAY, side).wait_recv()

            @pl.when(sp > 0)
            def _():
                block_copy(h, C, C, every, SIDE, side).wait_recv()

    def mix_copy(h):
        cols = pl.ds(pl.multiple_of((2 * h + tp) * HEAD, HEAD), HEAD)
        return remote(mixg.at[:, cols], mixg.at[:, cols], sent.at[MIX], mix_recv.at[h], across)

    eye = iota((block, block), 0) == iota((block, block), 1)

    def context(h, c, kind, first, last):
        return ctx[h, kind, c, first:last].reshape((last - first) * class_rows, HEAD)

    def visit(h, guest, bias, first, last, result, lse):
        for c in range(CLASSES):
            keys, vals = (context(h, c, kind, first, last) for kind in range(2))
            n, t, m = weighed(transposed_dot(guest[h, c], keys) * SCALE + bias, vals)
            result[h, c] = (n / t).astype(BF16)
            lse[h, c:c + 1, :] = jnp.sum(jnp.where(eye, m + jnp.log2(t), 0.0), axis=0, keepdims=True)

    def visit_far(h):
        meet(h, 0)

        @pl.when(has_next)
        def _():
            visit(h, visitor, visit_bias[...], A, O, part, part_lse)
        start_all(send_part(h))

    def visit_second(h):
        @pl.when(has_second)
        def _():
            second_copy(h, every).wait_recv()
            visit(h, second, pair_bias[2], C, SLOTS, back, back_lse)
        start_all(send_back(h))

    def tail_of(h, kind):
        return [ctx[h, kind, c, C, class_rows - share:] for c in range(CLASSES)]

    def join(n, t, m, n2, t2, m2):
        most = jnp.maximum(m, m2)
        old, new = jnp.exp2(m - most), jnp.exp2(m2 - most)
        return n * old + n2 * new, t * old + t2 * new, most

    def visit_first(h):
        @pl.when(has_next)
        def _():
            keys, vals = (jnp.concatenate(tail_of(h, kind), axis=0) for kind in range(2))
            guest = jnp.concatenate([visitor[h, c, :share] for c in range(CLASSES)], axis=0)
            close = weighed(transposed_dot(guest, keys) * SCALE + band[3, :, :block], vals)
            for c in range(CLASSES):
                keys, vals = (context(h, c, kind, C, SLOTS) for kind in range(2))
                n, t, m = weighed(transposed_dot(visitor[h, c], keys) * SCALE + pair_bias[1], vals)
                m = jnp.broadcast_to(m, (block, HEAD))
                vnum[h, c], vtot[h, c], vtop[h, c] = n, t, m
                n, t, m = join(n[:share], t[:share], m[:share], *(v[c * share:(c + 1) * share] for v in close))
                vnum[h, c, :share], vtot[h, c, :share], vtop[h, c, :share] = n, t, m

    def with_far(n, t, m, result, lse_row):
        lf = jnp.sum(jnp.where(eye, lse_row, 0.0), axis=1, keepdims=True)
        most = jnp.maximum(m, lf)
        en, ef = jnp.exp2(m - most), jnp.exp2(lf - most)
        total = t * en + ef
        return (n * en + result.astype(F32) * ef) / total, total, most

    def merge(h):
        @pl.when(has_next)
        def _():
            @pl.when(z > 0)
            def _():
                for copy in back_copies(h):
                    copy.wait_recv()
            for c in range(CLASSES):
                r, t, m = with_far(vnum[h, c], vtot[h, c], vtop[h, c], mid_out[h, c], mid_lse[h, c:c + 1, :])
                part[h, c] = r.astype(BF16)
                part_lse[h, c:c + 1, :] = jnp.sum(jnp.where(eye, m + jnp.log2(t), 0.0), axis=0, keepdims=True)
        start_all(send_part(h))

    def attend(h):
        first, bias, close = (C, pair_bias[0], band[2]) if h < guests else (A, far_bias[...], band[0])
        keys, vals = (jnp.concatenate(tail_of(h, kind) + [nat[h, :block]], axis=0)
                      for kind, nat in ((0, kn), (1, vn)))
        near(h, 0, keys, vals, close)
        for c in range(CLASSES):
            keys, vals = (context(h, c, kind, first, SLOTS) for kind in range(2))
            n, t, m = weighed(transposed_dot(q[h, c], keys) * SCALE + bias, vals)
            span = classed(h * rows, class_rows, c)
            cnum[h, c], ctot[h, c], ctop[h, c] = join(num[span, :], tot[span, :], top[span, :], n, t, m)

    def combine(h, _):
        @pl.when(z > 0)
        def _():
            for copy in part_copies(h):
                copy.wait_recv()

        for c in range(CLASSES):
            mixed, _, _ = with_far(cnum[h, c], ctot[h, c], ctop[h, c], far_out[h, c], far_lse[h, pl.ds(c, 1), :])
            mixf[classed(0, class_rows, c), :] = mixed
        cols = pl.ds(pl.multiple_of((2 * h + tp) * HEAD, HEAD), HEAD)
        mixg[:, cols] = mixf[...].astype(BF16)
        mix_copy(h).start()
        return 0

    def gathered(h, _):
        mix_copy(h).wait_recv()
        return 0

    out_cols = out_ref.shape[1]
    wide = 256

    def add_last(t, into):
        span = pl.ds(pl.multiple_of((2 * (heads - 1) + t) * HEAD, HEAD), HEAD)
        for i in range(out_cols // wide):
            cols = pl.ds(i * wide, wide)
            total = jnp.dot(mixg[:, span], wo[span, cols], preferred_element_type=F32)
            into[:, cols] = (out_sum[:, cols] + total).astype(into.dtype)

    def partial_out():
        most_in = (heads - 1) * 2 * HEAD
        for i in range(out_cols // wide):
            cols = pl.ds(i * wide, wide)
            out_sum[:, cols] = jnp.dot(mixg[:, :most_in], wo[:most_in, cols], preferred_element_type=F32)

    def ask(h, half):
        @pl.when(z > 0)
        def _():
            query_copy(h, half).start()

    load_kv(guests)
    project_kv(guests, tp)
    q_copies[0].wait()
    project_q(0, tp)
    for h in range(guests):
        ask(h, tp)
    load_kv(0)
    project_kv(0, tp)
    lax.fori_loop(other * PIECES, other * PIECES + PIECES, table, 0)
    x_copy.wait_recv()
    project_kv(guests, other)
    project_q(0, other)
    ask(0, other)
    project_kv(0, other)

    def project_rest(i, _):
        late = heads - guests - 1
        h = jnp.where(i < late, guests + 1 + i, i - late + 1)
        load_kv(h)
        project_kv(h, None)
        for g in range(1, guests):
            @pl.when(i == g - 1)
            def _():
                ask(g, other)
        return 0

    lax.fori_loop(0, heads - 2, project_rest, 0)
    for h in range(guests, heads):
        for half in order:
            start_all(send_side(h, half))
    meet(0, tp)
    masks()
    meet(0, other)
    for h in range(1, guests):
        meet(h, tp)
    near_inner(0)
    near_inner(1)
    neighbours(0)
    visit_first(0)
    for h in range(1, guests):
        meet(h, other)
    poll(guests)
    attend(0)
    for p in range(1, heads // 2):
        q_copies[p].wait()
        project_q(p, None)
    visit_second(0)
    for h in range(guests, heads):
        ask(h, 0)
    for h in range(1, guests):
        poll(guests + h)
        near_inner(guests)
        neighbours(h)
        visit_second(h)
        visit_first(h)
        attend(h)
    for h in range(2 * guests, heads):
        poll(h)
    for h in range(guests + 1, heads):
        near_inner(h)
    for h in range(guests):
        merge(h)
    for h in range(guests, heads):
        neighbours(h)
        visit_far(h)
        attend(h)
        if h < heads - 1:
            combine(h - guests, 0)
    for h in range(heads - guests - 1, heads - 1):
        combine(h, 0)
    pltpu.make_async_copy(wo_hbm, wo, wo_sem.at[0]).wait()
    for h in range(heads - 1):
        gathered(h, 0)
    partial_out()
    combine(heads - 1, 0)
    add_last(tp, out_sum)
    gathered(heads - 1, 0)
    add_last(other, out_ref)

    x_copy.wait_send()
    firsts, rest = pl.ds(0, guests), pl.ds(guests, heads - guests)
    for condition, ref, kind in (
        (has_next, ctx.at[rest, :, :, O], DOWN),
        (even, ctx.at[:, :, :, O], SIDE),
        (odd == 1, ctx.at[firsts, :, :, O], SIDE),
        ((odd == 1) & (z > 0), ctx.at[rest, :, :, A], RELAY),
        (z > 0, q, ASK),
        (has_next & (z > 0), visitor.at[firsts], SECOND),
        (has_next, part, PART),
        (has_next, part_lse, LSE),
        (has_second, back, MID),
        (has_second, back_lse, MID_LSE),
    ):
        @pl.when(condition)
        def _():
            remote(ref, ref, sent.at[kind], x_sem.at[1], side).wait_send()
    half_mix = mixg.at[:, pl.ds(0, heads * HEAD)]
    remote(half_mix, half_mix, sent.at[MIX], x_sem.at[1], across).wait_send()


def body(tokens, query_weight, key_weight, value_weight, output_weight):
    n_sp = lax.axis_size("sp")
    half_rows, width = tokens.shape
    rows = half_rows * lax.axis_size("tp")
    heads = query_weight.shape[1] // HEAD
    assert rows * 4 == FAR_DILATION * REACH_STEPS and rows == 512
    assert n_sp % 2 == 0 and lax.axis_size("tp") == 2 and heads % 2 == 0 and heads >= 4

    half = HEAD // 2
    inverse = THETA_BASE ** (-np.arange(half, dtype=np.float64) / half)
    inverse = np.concatenate([inverse, inverse]).astype(np.float32)[None, :]

    guests = heads // 2
    class_rows = rows // CLASSES
    anywhere = pl.BlockSpec(memory_space=pl.ANY)
    vmem = pl.BlockSpec(memory_space=pltpu.VMEM)
    out_cols = output_weight.shape[1]
    dma = pltpu.SemaphoreType.DMA
    return pl.pallas_call(
        functools.partial(kernel, n_sp, heads, guests),
        out_shape=pltpu.VMEM((rows, out_cols), BF16),
        in_specs=[anywhere] * 6,
        out_specs=vmem,
        scratch_shapes=[
            pltpu.VMEM((2, half_rows, width), BF16),
            pltpu.VMEM((heads, width, 2 * HEAD), BF16),
            pltpu.VMEM((heads // 2, width, 2 * HEAD), BF16),
            pltpu.VMEM(output_weight.shape, BF16),
            pltpu.VMEM((1, HEAD), F32),
            pltpu.VMEM((rows, HEAD), F32),
            pltpu.VMEM((rows, HEAD), F32),
            pltpu.VMEM((heads, 2, CLASSES, SLOTS, class_rows, HEAD), BF16),
            pltpu.VMEM((heads, CLASSES, class_rows, HEAD), BF16),
            pltpu.VMEM((heads, rows, HEAD), BF16),
            pltpu.VMEM((heads, rows, HEAD), BF16),
            pltpu.VMEM((heads, rows, HEAD), BF16),
            pltpu.VMEM((heads, CLASSES, class_rows, HEAD), BF16),
            pltpu.VMEM((guests, CLASSES, class_rows, HEAD), BF16),
            pltpu.VMEM((rows, HEAD), F32),
            pltpu.VMEM((rows, HEAD), F32),
            pltpu.VMEM((REACH_STEPS, SLOTS * REACH_STEPS), F32),
            pltpu.VMEM((REACH_STEPS, 2 * REACH_STEPS), F32),
            pltpu.VMEM((3, REACH_STEPS, 2 * REACH_STEPS), F32),
            pltpu.VMEM((4, REACH_STEPS, 2 * REACH_STEPS), F32),
            pltpu.VMEM((heads * rows, HEAD), F32),
            pltpu.VMEM((heads * rows, HEAD), F32),
            pltpu.VMEM((heads * rows, HEAD), F32),
            pltpu.VMEM((heads, CLASSES, class_rows, HEAD), F32),
            pltpu.VMEM((heads, CLASSES, class_rows, HEAD), F32),
            pltpu.VMEM((heads, CLASSES, class_rows, HEAD), F32),
            pltpu.VMEM((guests, CLASSES, class_rows, HEAD), F32),
            pltpu.VMEM((guests, CLASSES, class_rows, HEAD), F32),
            pltpu.VMEM((guests, CLASSES, class_rows, HEAD), F32),
            pltpu.VMEM((heads, CLASSES, class_rows, HEAD), BF16),
            pltpu.VMEM((heads, 8, 128), F32),
            pltpu.VMEM((heads, CLASSES, class_rows, HEAD), BF16),
            pltpu.VMEM((heads, 8, 128), F32),
            pltpu.VMEM((guests, CLASSES, class_rows, HEAD), BF16),
            pltpu.VMEM((guests, 8, 128), F32),
            pltpu.VMEM((guests, CLASSES, class_rows, HEAD), BF16),
            pltpu.VMEM((guests, 8, 128), F32),
            pltpu.VMEM((rows, HEAD), F32),
            pltpu.VMEM((rows, 2 * heads * HEAD), BF16),
            pltpu.VMEM((rows, out_cols), F32),
            dma((1,)),
            dma((1,)),
            dma((heads,)),
            dma((heads // 2,)),
            dma((1,)),
            dma((2,)),
            dma((10,)),
            dma((heads - guests,)),
            dma((heads,)),
            dma((heads + guests,)),
            dma((guests,)),
            dma((heads,)),
            dma((heads,)),
            dma((guests,)),
            dma((guests,)),
            dma((heads,)),
        ],
        compiler_params=pltpu.CompilerParams(
            collective_id=0, has_side_effects=True, vmem_limit_bytes=56 * 1024 * 1024
        ),
    )(tokens, query_weight, key_weight, value_weight, output_weight, jnp.asarray(inverse))


def solution(mesh):
    in_specs = (
        P(("grp", "sp", "tp"), None),
        P(None, "tp"),
        P(None, "tp"),
        P(None, "tp"),
        P(None, "tp"),
    )
    out_specs = P(("grp", "sp"), "tp")
    return jax.shard_map(body, mesh=mesh, in_specs=in_specs, out_specs=out_specs, check_vma=False)
```

```python
import functools

import jax
import jax.numpy as jnp
import numpy as np
from jax import lax
from jax.experimental import pallas as pl
from jax.experimental.pallas import tpu as pltpu
from jax.sharding import PartitionSpec as P

HEAD = 128
REACH_STEPS = 128
MIDDLE_DILATION = 4
FAR_DILATION = 16
THETA_BASE = 500000.0
NEG = -1e30
MESH = pl.DeviceIdType.MESH
F32 = jnp.float32
BF16 = jnp.bfloat16
SCALE = HEAD ** -0.5 / float(np.log(2.0))

A, C, O = 0, 1, 2
SLOTS = 3
CLASSES = MIDDLE_DILATION
PIECES = 2


def iota(shape, dim):
    return lax.broadcasted_iota(jnp.int32, shape, dim)


def rotated(x, cosine, sine):
    return x * cosine + pltpu.roll(x, HEAD // 2, 1) * sine


def weighed(scores, values):
    top = jnp.max(scores, axis=-1, keepdims=True)
    raised = jnp.exp2(scores - top).astype(BF16)
    ones = jnp.ones(values.shape, BF16)
    both = jnp.dot(raised, jnp.concatenate([values, ones], axis=1), preferred_element_type=F32)
    return both[:, :HEAD], both[:, HEAD:], top


def transposed_dot(a, b):
    return lax.dot_general(a, b, (((1,), (1,)), ((), ())), preferred_element_type=F32)


def classed(start, count, c):
    return pl.ds(start + c, count, stride=CLASSES)


def kernel(
    n_sp, heads, guests,
    tok_hbm, wq_hbm, wk_hbm, wv_hbm, wo_hbm,
    out_ref,
    x, wkv, wq, wo, cos_ref, sin_ref, ctx, q, qn, kn, vn, visitor, second, flat_a, flat_b,
    far_bias, visit_bias, pair_bias, band, num, tot, top, cnum, ctot, ctop, vnum, vtot, vtop,
    part, part_lse, far_out, far_lse, back, back_lse, mid_out, mid_lse, mixf, mixg, out_sum,
    tok_sem, kv_sem, q_load, wo_sem, x_sem, sent,
    a_recv, c_recv, q_recv, second_recv, part_recv, lse_recv, mid_recv, mid_lse_recv, mix_recv,
):
    sp = lax.axis_index("sp")
    tp = lax.axis_index("tp")
    z = sp // 2
    odd = sp % 2
    even = odd == 0
    other = 1 - tp
    has_next = z + 1 < n_sp // 2
    has_second = z + 2 < n_sp // 2
    half_rows = x.shape[1]
    rows = 2 * half_rows
    class_rows = rows // CLASSES
    half_class = class_rows // 2
    piece = half_rows // PIECES
    order = (tp, other)

    tok_copy = pltpu.make_async_copy(tok_hbm, x.at[tp], tok_sem.at[0])
    tok_copy.start()

    def kv_copy(h, kind):
        source = (wk_hbm, wv_hbm)[kind]
        cols = pl.ds(h * HEAD, HEAD)
        return pltpu.make_async_copy(source.at[:, cols], wkv.at[h, :, pl.ds(kind * HEAD, HEAD)], kv_sem.at[h])

    q_copies = [
        pltpu.make_async_copy(wq_hbm.at[:, pl.ds(p * 2 * HEAD, 2 * HEAD)], wq.at[p], q_load.at[p])
        for p in range(heads // 2)]
    for kind in range(2):
        kv_copy(guests, kind).start()
    wo_copies = [
        pltpu.make_async_copy(
            wo_hbm.at[pl.ds((t * heads + h) * HEAD, HEAD)], wo.at[pl.ds((2 * h + t) * HEAD, HEAD)], wo_sem.at[0])
        for h in range(heads) for t in range(2)]

    barrier = pltpu.get_barrier_semaphore()
    y_partner = sp + 1 - 2 * odd

    def greet(ids):
        pl.semaphore_signal(barrier, inc=1, device_id=ids, device_id_type=MESH)

    greet({"tp": other})
    greet({"sp": y_partner})

    @pl.when(has_next)
    def _():
        greet({"sp": sp + 2})

    @pl.when(z > 0)
    def _():
        greet({"sp": sp - 2})

    def remote(src, dst, send_sem, recv_sem, ids):
        return pltpu.make_async_remote_copy(
            src_ref=src, dst_ref=dst, send_sem=send_sem, recv_sem=recv_sem,
            device_id=ids, device_id_type=MESH)

    down = {"sp": sp + 2}
    up = {"sp": sp - 2}
    side = {"sp": y_partner}
    across = {"tp": other}

    block = REACH_STEPS
    share = block // CLASSES
    ratio = FAR_DILATION // MIDDLE_DILATION

    def masks():
        qi, kj = iota((block, SLOTS * block), 0), iota((block, SLOTS * block), 1)
        slot = kj // block
        apart = qi - (kj % block)

        def bias(dist, here):
            steps = apart + block * dist
            mid = here & (steps >= 0) & (steps <= REACH_STEPS)
            far = here & (steps >= 0) & (steps % ratio == 0) & (steps <= ratio * REACH_STEPS)
            return jnp.where(mid & far, 1.0, jnp.where(mid | far, 0.0, NEG))

        far_bias[...] = bias(O - slot, O - slot <= sp)
        visit_bias[...] = bias(O + 2 - slot, O - slot <= sp)[:, :O * block]
        pair_bias[0] = bias(O - slot, (slot == O) | (odd == 1))[:, C * block:]
        pair_bias[1] = bias(jnp.where(slot == O, 2, 1 + 2 * odd), slot >= C)[:, C * block:]
        pair_bias[2] = bias(jnp.where(slot == O, 4, 3 + 2 * odd), slot >= C)[:, C * block:]
        ni, nj = iota((block, 2 * block), 0), iota((block, 2 * block), 1)
        gap = ni + block - nj
        band[1] = jnp.where((gap >= 0) & (gap <= REACH_STEPS), 0.0, NEG)
        gap = jnp.where(nj < block, ni + block - ((nj % share) * CLASSES + nj // share), gap)
        near_ok = (gap >= 0) & (gap <= REACH_STEPS)
        band[0] = jnp.where(near_ok & ((nj >= block) | (sp > 0)), 0.0, NEG)
        band[2] = jnp.where(near_ok & ((nj >= block) | (odd == 1)), 0.0, NEG)
        gap = ((ni % share) - (nj % share)) * CLASSES + ni // share - nj // share + block
        band[3] = jnp.where((gap >= 0) & (gap <= REACH_STEPS) & even & (nj < block), 0.0, NEG)

        for slot_at in (A, C):
            @pl.when(sp < 2 - slot_at)
            def _():
                def clear(h, _):
                    ctx[h, :, :, slot_at] = jnp.zeros((2, CLASSES, class_rows, HEAD), BF16)
                    return 0
                lax.fori_loop(guests, heads, clear, 0)

        part_lse[...] = jnp.zeros(part_lse.shape, F32)
        back_lse[...] = jnp.zeros(back_lse.shape, F32)

        @pl.when(z == 0)
        def _():
            far_out[...] = jnp.zeros(far_out.shape, BF16)
            far_lse[...] = jnp.full(far_lse.shape, NEG, F32)
            mid_out[...] = jnp.zeros(mid_out.shape, BF16)
            mid_lse[...] = jnp.full(mid_lse.shape, NEG, F32)

    lane = iota((piece, HEAD), 1)
    low = lane < HEAD // 2
    power = (iota((1, HEAD), 1) % (HEAD // 2)).astype(F32)
    inverse = jnp.exp2(power * (-2.0 * float(np.log2(THETA_BASE)) / HEAD))

    def table(c, _):
        start = pl.multiple_of(c * piece, piece)
        places = start + iota((piece, HEAD), 0) + half_rows * jnp.where(low, tp, other)
        angles = (sp * rows + places).astype(F32) * inverse
        cosine, sine = jnp.cos(angles), jnp.sin(angles)
        cosine_moved, sine_moved = pltpu.roll(cosine, HEAD // 2, 1), pltpu.roll(sine, HEAD // 2, 1)
        own = pl.ds(pl.multiple_of(tp * half_rows + start, piece), piece)
        rest = pl.ds(pl.multiple_of(other * half_rows + start, piece), piece)
        cos_ref[own, :] = jnp.where(low, cosine, cosine_moved)
        sin_ref[own, :] = jnp.where(low, -sine, sine_moved)
        cos_ref[rest, :] = jnp.where(low, cosine_moved, cosine)
        sin_ref[rest, :] = jnp.where(low, -sine_moved, sine)
        return 0

    lax.fori_loop(0, PIECES, table, 0)
    q_copies[0].start()
    for kind in range(2):
        kv_copy(0, kind).start()

    def load_kv(h):
        pltpu.make_async_copy(wk_hbm.at[:, pl.ds(0, 2 * HEAD)], wkv.at[h], kv_sem.at[h]).wait()

    def raw_kv(source, h, count):
        kv = jnp.dot(source, wkv[h], preferred_element_type=F32)
        flat_a[0:count] = kv[:, :HEAD]
        flat_b[0:count] = kv[:, HEAD:]

    tok_copy.wait()

    pl.semaphore_wait(barrier, 2 + has_next.astype(jnp.int32) + (z > 0).astype(jnp.int32))

    x_copy = remote(x.at[tp], x.at[tp], x_sem.at[0], x_sem.at[1], across)
    x_copy.start()
    for h in (*range(guests + 1, heads), *range(1, guests)):
        for kind in range(2):
            kv_copy(h, kind).start()
    for copy in (*q_copies[1:], *wo_copies):
        copy.start()

    DOWN, SIDE, RELAY, ASK, SECOND, PART, LSE, MID, MID_LSE, MIX = range(10)

    def spots_of(half):
        return pl.ds(pl.multiple_of(half * half_class, half_class), half_class)

    def block_copy(h, src, dst, rows_at, kind, ids):
        arrived = a_recv.at[h - guests] if dst == A else c_recv.at[h]
        return remote(ctx.at[h, :, :, src, rows_at], ctx.at[h, :, :, dst, rows_at], sent.at[kind], arrived, ids)

    every = pl.ds(0, class_rows)

    def send_down(h, half):
        return ((has_next & (h >= guests), block_copy(jnp.maximum(h, guests), O, A, spots_of(half), DOWN, down)),)

    def send_side(h, half):
        return ((even | (h < guests), block_copy(h, O, C, spots_of(half), SIDE, side)),)

    def send_relay(h):
        return (((odd == 1) & (z > 0), block_copy(h, A, C, every, RELAY, side)),)

    def query_copy(h, half):
        rows_at, arrived = (spots_of(half), q_recv.at[2 * h + half]) if h < guests else (every, q_recv.at[guests + h])
        return remote(q.at[h, :, rows_at], visitor.at[h, :, rows_at], sent.at[ASK], arrived, up)

    def second_copy(h, rows_at):
        return remote(visitor.at[h, :, rows_at], second.at[h, :, rows_at], sent.at[SECOND], second_recv.at[h], up)

    def back_copies(h):
        return (remote(back.at[h], mid_out.at[h], sent.at[MID], mid_recv.at[h], down),
                remote(back_lse.at[h], mid_lse.at[h], sent.at[MID_LSE], mid_lse_recv.at[h], down))

    def part_copies(h):
        return (remote(part.at[h], far_out.at[h], sent.at[PART], part_recv.at[h], down),
                remote(part_lse.at[h], far_lse.at[h], sent.at[LSE], lse_recv.at[h], down))

    def send_back(h):
        return tuple((has_second, copy) for copy in back_copies(h))

    def send_part(h):
        return tuple((has_next, copy) for copy in part_copies(h))

    def start_all(sends):
        for condition, copy in sends:
            @pl.when(condition)
            def _():
                copy.start()

    def project_kv(h, half):
        if half is None:
            source, natural, count, spots = x[...].reshape(rows, x.shape[2]), pl.ds(0, rows), rows, every
        else:
            source, natural = x[half], pl.ds(pl.multiple_of(half * half_rows, half_rows), half_rows)
            count, spots = half_rows, spots_of(half)
        raw_kv(source, h, count)
        k = rotated(flat_a[0:count], cos_ref[natural], sin_ref[natural])
        flat_a[0:count] = k
        kn[h, natural] = k.astype(BF16)
        vn[h, natural] = flat_b[0:count].astype(BF16)
        for c in range(CLASSES):
            ctx[h, 0, c, O, spots] = flat_a[classed(0, count // CLASSES, c), :].astype(BF16)
            ctx[h, 1, c, O, spots] = flat_b[classed(0, count // CLASSES, c), :].astype(BF16)
        for part_half in (order if half is None else (half,)):
            start_all(send_down(h, part_half))
            for condition, copy in send_side(h, part_half):
                @pl.when(h < guests)
                def _():
                    copy.start()

    def project_q(p, half):
        if half is None:
            source, natural, count = x[...].reshape(rows, x.shape[2]), pl.ds(0, rows), rows
            spots = pl.ds(0, class_rows)
        else:
            source, natural = x[half], pl.ds(pl.multiple_of(half * half_rows, half_rows), half_rows)
            count, spots = half_rows, pl.ds(pl.multiple_of(half * half_class, half_class), half_class)
        qq = jnp.dot(source, wq[p], preferred_element_type=F32)
        for s, flat in ((0, flat_a), (1, flat_b)):
            r = rotated(qq[:, s * HEAD:(s + 1) * HEAD], cos_ref[natural], sin_ref[natural])
            flat[0:count] = r
            qn[2 * p + s, natural] = r.astype(BF16)
            for c in range(CLASSES):
                q[2 * p + s, c, spots] = flat[classed(0, count // CLASSES, c), :].astype(BF16)

    def near(h, b, keys, vals, bias):
        scores = transposed_dot(qn[h, b * block:(b + 1) * block], keys) * SCALE + bias
        n, t, m = weighed(scores, vals)
        span = pl.ds(pl.multiple_of(h * rows, rows) + b * block, block)
        num[span, :] = n
        tot[span, :] = t
        top[span, :] = jnp.broadcast_to(m, (block, HEAD))

    def near_inner(h):
        for b in range(1, rows // block):
            span = slice((b - 1) * block, (b + 1) * block)
            near(h, b, kn[h, span], vn[h, span], band[1])

    def poll(h):
        @pl.when((odd == 1) & (z > 0))
        def _():
            block_copy(h, A, A, every, RELAY, side).wait_recv()
        start_all(send_relay(h))

    def meet(h, half):
        @pl.when(has_next)
        def _():
            query_copy(h, half).wait_recv()
        if h < guests:
            @pl.when(has_next & (z > 0))
            def _():
                second_copy(h, spots_of(half)).start()

    def neighbours(h):
        if h < guests:
            block_copy(h, C, C, every, SIDE, side).wait_recv()
        else:
            @pl.when(even & (z > 0))
            def _():
                block_copy(h, A, A, every, RELAY, side).wait_recv()

            @pl.when(sp > 0)
            def _():
                block_copy(h, C, C, every, SIDE, side).wait_recv()

    def mix_copy(h):
        return remote(mixg.at[2 * h + tp], mixg.at[2 * h + tp], sent.at[MIX], mix_recv.at[h], across)

    eye = iota((block, block), 0) == iota((block, block), 1)

    def context(h, c, kind, first, last):
        return ctx[h, kind, c, first:last].reshape((last - first) * class_rows, HEAD)

    def visit(h, guest, bias, first, last, result, lse):
        for c in range(CLASSES):
            keys, vals = (context(h, c, kind, first, last) for kind in range(2))
            n, t, m = weighed(transposed_dot(guest[h, c], keys) * SCALE + bias, vals)
            result[h, c] = (n / t).astype(BF16)
            lse[h, c:c + 1, :] = jnp.sum(jnp.where(eye, m + jnp.log2(t), 0.0), axis=0, keepdims=True)

    def visit_far(h):
        meet(h, 0)

        @pl.when(has_next)
        def _():
            visit(h, visitor, visit_bias[...], A, O, part, part_lse)
        start_all(send_part(h))

    def visit_second(h):
        @pl.when(has_second)
        def _():
            second_copy(h, every).wait_recv()
            visit(h, second, pair_bias[2], C, SLOTS, back, back_lse)
        start_all(send_back(h))

    def tail_of(h, kind):
        return [ctx[h, kind, c, C, class_rows - share:] for c in range(CLASSES)]

    def join(n, t, m, n2, t2, m2):
        most = jnp.maximum(m, m2)
        old, new = jnp.exp2(m - most), jnp.exp2(m2 - most)
        return n * old + n2 * new, t * old + t2 * new, most

    def visit_first(h):
        @pl.when(has_next)
        def _():
            keys, vals = (jnp.concatenate(tail_of(h, kind), axis=0) for kind in range(2))
            guest = jnp.concatenate([visitor[h, c, :share] for c in range(CLASSES)], axis=0)
            close = weighed(transposed_dot(guest, keys) * SCALE + band[3, :, :block], vals)
            for c in range(CLASSES):
                keys, vals = (context(h, c, kind, C, SLOTS) for kind in range(2))
                n, t, m = weighed(transposed_dot(visitor[h, c], keys) * SCALE + pair_bias[1], vals)
                m = jnp.broadcast_to(m, (block, HEAD))
                vnum[h, c], vtot[h, c], vtop[h, c] = n, t, m
                n, t, m = join(n[:share], t[:share], m[:share], *(v[c * share:(c + 1) * share] for v in close))
                vnum[h, c, :share], vtot[h, c, :share], vtop[h, c, :share] = n, t, m

    def with_far(n, t, m, result, lse_row):
        lf = jnp.sum(jnp.where(eye, lse_row, 0.0), axis=1, keepdims=True)
        most = jnp.maximum(m, lf)
        en, ef = jnp.exp2(m - most), jnp.exp2(lf - most)
        total = t * en + ef
        return (n * en + result.astype(F32) * ef) / total, total, most

    def merge(h):
        @pl.when(has_next)
        def _():
            @pl.when(z > 0)
            def _():
                for copy in back_copies(h):
                    copy.wait_recv()
            for c in range(CLASSES):
                r, t, m = with_far(vnum[h, c], vtot[h, c], vtop[h, c], mid_out[h, c], mid_lse[h, c:c + 1, :])
                part[h, c] = r.astype(BF16)
                part_lse[h, c:c + 1, :] = jnp.sum(jnp.where(eye, m + jnp.log2(t), 0.0), axis=0, keepdims=True)
        start_all(send_part(h))

    def attend(h):
        first, bias, close = (C, pair_bias[0], band[2]) if h < guests else (A, far_bias[...], band[0])
        keys, vals = (jnp.concatenate(tail_of(h, kind) + [nat[h, :block]], axis=0)
                      for kind, nat in ((0, kn), (1, vn)))
        near(h, 0, keys, vals, close)
        for c in range(CLASSES):
            keys, vals = (context(h, c, kind, first, SLOTS) for kind in range(2))
            n, t, m = weighed(transposed_dot(q[h, c], keys) * SCALE + bias, vals)
            span = classed(h * rows, class_rows, c)
            cnum[h, c], ctot[h, c], ctop[h, c] = join(num[span, :], tot[span, :], top[span, :], n, t, m)

    def combine(h, _):
        @pl.when(z > 0)
        def _():
            for copy in part_copies(h):
                copy.wait_recv()

        for c in range(CLASSES):
            mixed, _, _ = with_far(cnum[h, c], ctot[h, c], ctop[h, c], far_out[h, c], far_lse[h, pl.ds(c, 1), :])
            mixf[classed(0, class_rows, c), :] = mixed
        mixg[2 * h + tp] = mixf[...].astype(BF16)
        mix_copy(h).start()
        return 0

    def gathered(h, _):
        mix_copy(h).wait_recv()
        return 0

    out_cols = out_ref.shape[1]
    wide = 256

    def add_last(t, into):
        at = 2 * (heads - 1) + t
        span = pl.ds(pl.multiple_of(at * HEAD, HEAD), HEAD)
        for i in range(out_cols // wide):
            cols = pl.ds(i * wide, wide)
            total = jnp.dot(mixg[at], wo[span, cols], preferred_element_type=F32)
            into[:, cols] = (out_sum[:, cols] + total).astype(into.dtype)

    def partial_out():
        most = 2 * (heads - 1)
        mixed = jnp.concatenate([mixg[i] for i in range(most)], axis=1)
        for i in range(out_cols // wide):
            cols = pl.ds(i * wide, wide)
            out_sum[:, cols] = jnp.dot(mixed, wo[:most * HEAD, cols], preferred_element_type=F32)

    def ask(h, half):
        @pl.when(z > 0)
        def _():
            query_copy(h, half).start()

    load_kv(guests)
    project_kv(guests, tp)
    q_copies[0].wait()
    project_q(0, tp)
    for h in range(guests):
        ask(h, tp)
    load_kv(0)
    project_kv(0, tp)
    x_copy.wait_recv()
    project_kv(guests, other)
    project_q(0, other)
    ask(0, other)
    project_kv(0, other)

    def project_rest(i, _):
        late = heads - guests - 1
        h = jnp.where(i < late, guests + 1 + i, i - late + 1)
        load_kv(h)
        project_kv(h, None)
        for g in range(1, guests):
            @pl.when(i == g - 1)
            def _():
                ask(g, other)
        return 0

    lax.fori_loop(0, heads - 2, project_rest, 0)
    for h in range(guests, heads):
        for half in order:
            start_all(send_side(h, half))
    meet(0, tp)
    masks()
    meet(0, other)
    near_inner(0)
    near_inner(1)
    neighbours(0)
    for h in range(1, guests):
        meet(h, tp)
    visit_first(0)
    for h in range(1, guests):
        meet(h, other)
    poll(guests)
    attend(0)
    visit_second(0)
    for p in range(1, heads // 2):
        q_copies[p].wait()
        project_q(p, None)
    for h in range(guests, heads):
        ask(h, 0)
    for h in range(1, guests):
        poll(guests + h)
        near_inner(guests)
        neighbours(h)
        visit_second(h)
        visit_first(h)
        attend(h)
    for h in range(2 * guests, heads):
        poll(h)
    for h in range(guests + 1, heads):
        near_inner(h)
    for h in range(guests):
        merge(h)
    for h in range(guests, heads):
        neighbours(h)
        visit_far(h)
        attend(h)
        if h < heads - 1:
            combine(h - guests, 0)
    for h in range(heads - guests - 1, heads):
        combine(h, 0)
    pltpu.make_async_copy(wo_hbm, wo, wo_sem.at[0]).wait()
    for h in range(heads - 1):
        gathered(h, 0)
    partial_out()
    add_last(tp, out_sum)
    gathered(heads - 1, 0)
    add_last(other, out_ref)

    x_copy.wait_send()
    firsts, rest = pl.ds(0, guests), pl.ds(guests, heads - guests)
    for condition, ref, kind in (
        (has_next, ctx.at[rest, :, :, O], DOWN),
        (even, ctx.at[:, :, :, O], SIDE),
        (odd == 1, ctx.at[firsts, :, :, O], SIDE),
        ((odd == 1) & (z > 0), ctx.at[rest, :, :, A], RELAY),
        (z > 0, q, ASK),
        (has_next & (z > 0), visitor.at[firsts], SECOND),
        (has_next, part, PART),
        (has_next, part_lse, LSE),
        (has_second, back, MID),
        (has_second, back_lse, MID_LSE),
    ):
        @pl.when(condition)
        def _():
            remote(ref, ref, sent.at[kind], x_sem.at[1], side).wait_send()
    half_mix = mixg.at[pl.ds(0, heads)]
    remote(half_mix, half_mix, sent.at[MIX], x_sem.at[1], across).wait_send()


def body(tokens, query_weight, key_weight, value_weight, output_weight):
    n_sp = lax.axis_size("sp")
    half_rows, width = tokens.shape
    rows = half_rows * lax.axis_size("tp")
    heads = query_weight.shape[1] // HEAD
    assert rows * 4 == FAR_DILATION * REACH_STEPS and rows == 512
    assert n_sp % 2 == 0 and lax.axis_size("tp") == 2 and heads % 2 == 0 and heads >= 4

    guests = heads // 2
    class_rows = rows // CLASSES
    anywhere = pl.BlockSpec(memory_space=pl.ANY)
    vmem = pl.BlockSpec(memory_space=pltpu.VMEM)
    out_cols = output_weight.shape[1]
    dma = pltpu.SemaphoreType.DMA
    return pl.pallas_call(
        functools.partial(kernel, n_sp, heads, guests),
        out_shape=pltpu.VMEM((rows, out_cols), BF16),
        in_specs=[anywhere] * 5,
        out_specs=vmem,
        scratch_shapes=[
            pltpu.VMEM((2, half_rows, width), BF16),
            pltpu.VMEM((heads, width, 2 * HEAD), BF16),
            pltpu.VMEM((heads // 2, width, 2 * HEAD), BF16),
            pltpu.VMEM(output_weight.shape, BF16),
            pltpu.VMEM((rows, HEAD), F32),
            pltpu.VMEM((rows, HEAD), F32),
            pltpu.VMEM((heads, 2, CLASSES, SLOTS, class_rows, HEAD), BF16),
            pltpu.VMEM((heads, CLASSES, class_rows, HEAD), BF16),
            pltpu.VMEM((heads, rows, HEAD), BF16),
            pltpu.VMEM((heads, rows, HEAD), BF16),
            pltpu.VMEM((heads, rows, HEAD), BF16),
            pltpu.VMEM((heads, CLASSES, class_rows, HEAD), BF16),
            pltpu.VMEM((guests, CLASSES, class_rows, HEAD), BF16),
            pltpu.VMEM((rows, HEAD), F32),
            pltpu.VMEM((rows, HEAD), F32),
            pltpu.VMEM((REACH_STEPS, SLOTS * REACH_STEPS), F32),
            pltpu.VMEM((REACH_STEPS, 2 * REACH_STEPS), F32),
            pltpu.VMEM((3, REACH_STEPS, 2 * REACH_STEPS), F32),
            pltpu.VMEM((4, REACH_STEPS, 2 * REACH_STEPS), F32),
            pltpu.VMEM((heads * rows, HEAD), F32),
            pltpu.VMEM((heads * rows, HEAD), F32),
            pltpu.VMEM((heads * rows, HEAD), F32),
            pltpu.VMEM((heads, CLASSES, class_rows, HEAD), F32),
            pltpu.VMEM((heads, CLASSES, class_rows, HEAD), F32),
            pltpu.VMEM((heads, CLASSES, class_rows, HEAD), F32),
            pltpu.VMEM((guests, CLASSES, class_rows, HEAD), F32),
            pltpu.VMEM((guests, CLASSES, class_rows, HEAD), F32),
            pltpu.VMEM((guests, CLASSES, class_rows, HEAD), F32),
            pltpu.VMEM((heads, CLASSES, class_rows, HEAD), BF16),
            pltpu.VMEM((heads, 8, 128), F32),
            pltpu.VMEM((heads, CLASSES, class_rows, HEAD), BF16),
            pltpu.VMEM((heads, 8, 128), F32),
            pltpu.VMEM((guests, CLASSES, class_rows, HEAD), BF16),
            pltpu.VMEM((guests, 8, 128), F32),
            pltpu.VMEM((guests, CLASSES, class_rows, HEAD), BF16),
            pltpu.VMEM((guests, 8, 128), F32),
            pltpu.VMEM((rows, HEAD), F32),
            pltpu.VMEM((2 * heads, rows, HEAD), BF16),
            pltpu.VMEM((rows, out_cols), F32),
            dma((1,)),
            dma((heads,)),
            dma((heads // 2,)),
            dma((1,)),
            dma((2,)),
            dma((10,)),
            dma((heads - guests,)),
            dma((heads,)),
            dma((heads + guests,)),
            dma((guests,)),
            dma((heads,)),
            dma((heads,)),
            dma((guests,)),
            dma((guests,)),
            dma((heads,)),
        ],
        compiler_params=pltpu.CompilerParams(
            collective_id=0, has_side_effects=True, vmem_limit_bytes=56 * 1024 * 1024
        ),
    )(tokens, query_weight, key_weight, value_weight, output_weight)


def solution(mesh):
    in_specs = (
        P(("grp", "sp", "tp"), None),
        P(None, "tp"),
        P(None, "tp"),
        P(None, "tp"),
        P(None, "tp"),
    )
    out_specs = P(("grp", "sp"), "tp")
    return jax.shard_map(body, mesh=mesh, in_specs=in_specs, out_specs=out_specs, check_vma=False)
```

```python
import functools

import jax
import jax.numpy as jnp
import numpy as np
from jax import lax
from jax.experimental import pallas as pl
from jax.experimental.pallas import tpu as pltpu
from jax.sharding import PartitionSpec as P

HEAD = 128
REACH_STEPS = 128
MIDDLE_DILATION = 4
FAR_DILATION = 16
THETA_BASE = 500000.0
NEG = -1e30
MESH = pl.DeviceIdType.MESH
F32 = jnp.float32
BF16 = jnp.bfloat16
SCALE = HEAD ** -0.5 / float(np.log(2.0))

A, C, O = 0, 1, 2
SLOTS = 3
CLASSES = MIDDLE_DILATION
PIECES = 2


def iota(shape, dim):
    return lax.broadcasted_iota(jnp.int32, shape, dim)


def rotated(x, cosine, sine):
    return x * cosine + pltpu.roll(x, HEAD // 2, 1) * sine


def weighed(scores, values):
    top = jnp.max(scores, axis=-1, keepdims=True)
    raised = jnp.exp2(scores - top).astype(BF16)
    ones = jnp.ones(values.shape, BF16)
    both = jnp.dot(raised, jnp.concatenate([values, ones], axis=1), preferred_element_type=F32)
    return both[:, :HEAD], both[:, HEAD:], top


def transposed_dot(a, b):
    return lax.dot_general(a, b, (((1,), (1,)), ((), ())), preferred_element_type=F32)


def classed(start, count, c):
    return pl.ds(start + c, count, stride=CLASSES)


def kernel(
    n_sp, heads, guests,
    tok_hbm, wq_hbm, wk_hbm, wv_hbm, wo_hbm,
    out_ref,
    x, wkv, wq, wo, cos_ref, sin_ref, ctx, q, qn, kn, vn, visitor, second, flat_a, flat_b,
    far_bias, visit_bias, pair_bias, band, num, tot, top, cnum, ctot, ctop, vnum, vtot, vtop,
    part, part_lse, far_out, far_lse, back, back_lse, mid_out, mid_lse, mixf, mixg, out_sum,
    tok_sem, kv_sem, q_load, wo_sem, x_sem, sent,
    a_recv, c_recv, q_recv, second_recv, part_recv, mid_recv, mix_recv,
):
    sp = lax.axis_index("sp")
    tp = lax.axis_index("tp")
    z = sp // 2
    odd = sp % 2
    even = odd == 0
    other = 1 - tp
    has_next = z + 1 < n_sp // 2
    has_second = z + 2 < n_sp // 2
    half_rows = x.shape[1]
    rows = 2 * half_rows
    class_rows = rows // CLASSES
    half_class = class_rows // 2
    piece = half_rows // PIECES
    order = (tp, other)

    tok_copy = pltpu.make_async_copy(tok_hbm, x.at[tp], tok_sem.at[0])
    tok_copy.start()

    def kv_copy(h, kind):
        source = (wk_hbm, wv_hbm)[kind]
        cols = pl.ds(h * HEAD, HEAD)
        return pltpu.make_async_copy(source.at[:, cols], wkv.at[h, :, pl.ds(kind * HEAD, HEAD)], kv_sem.at[h])

    q_copies = [
        pltpu.make_async_copy(wq_hbm.at[:, pl.ds(p * 2 * HEAD, 2 * HEAD)], wq.at[p], q_load.at[p])
        for p in range(heads // 2)]
    for kind in range(2):
        kv_copy(guests, kind).start()
    wo_copies = [
        pltpu.make_async_copy(
            wo_hbm.at[pl.ds((t * heads + h) * HEAD, HEAD)], wo.at[pl.ds((2 * h + t) * HEAD, HEAD)], wo_sem.at[0])
        for h in range(heads) for t in range(2)]

    barrier = pltpu.get_barrier_semaphore()
    y_partner = sp + 1 - 2 * odd

    def greet(ids):
        pl.semaphore_signal(barrier, inc=1, device_id=ids, device_id_type=MESH)

    greet({"tp": other})
    greet({"sp": y_partner})

    @pl.when(has_next)
    def _():
        greet({"sp": sp + 2})

    @pl.when(z > 0)
    def _():
        greet({"sp": sp - 2})

    def remote(src, dst, send_sem, recv_sem, ids):
        return pltpu.make_async_remote_copy(
            src_ref=src, dst_ref=dst, send_sem=send_sem, recv_sem=recv_sem,
            device_id=ids, device_id_type=MESH)

    down = {"sp": sp + 2}
    up = {"sp": sp - 2}
    side = {"sp": y_partner}
    across = {"tp": other}

    block = REACH_STEPS
    share = block // CLASSES
    ratio = FAR_DILATION // MIDDLE_DILATION

    def masks():
        qi, kj = iota((block, SLOTS * block), 0), iota((block, SLOTS * block), 1)
        slot = kj // block
        apart = qi - (kj % block)

        def bias(dist, here):
            steps = apart + block * dist
            mid = here & (steps >= 0) & (steps <= REACH_STEPS)
            far = here & (steps >= 0) & (steps % ratio == 0) & (steps <= ratio * REACH_STEPS)
            return jnp.where(mid & far, 1.0, jnp.where(mid | far, 0.0, NEG))

        far_bias[...] = bias(O - slot, O - slot <= sp)
        visit_bias[...] = bias(O + 2 - slot, O - slot <= sp)[:, :O * block]
        pair_bias[0] = bias(O - slot, (slot == O) | (odd == 1))[:, C * block:]
        pair_bias[1] = bias(jnp.where(slot == O, 2, 1 + 2 * odd), slot >= C)[:, C * block:]
        pair_bias[2] = bias(jnp.where(slot == O, 4, 3 + 2 * odd), slot >= C)[:, C * block:]
        ni, nj = iota((block, 2 * block), 0), iota((block, 2 * block), 1)
        gap = ni + block - nj
        band[1] = jnp.where((gap >= 0) & (gap <= REACH_STEPS), 0.0, NEG)
        gap = jnp.where(nj < block, ni + block - ((nj % share) * CLASSES + nj // share), gap)
        near_ok = (gap >= 0) & (gap <= REACH_STEPS)
        band[0] = jnp.where(near_ok & ((nj >= block) | (sp > 0)), 0.0, NEG)
        band[2] = jnp.where(near_ok & ((nj >= block) | (odd == 1)), 0.0, NEG)
        gap = ((ni % share) - (nj % share)) * CLASSES + ni // share - nj // share + block
        band[3] = jnp.where((gap >= 0) & (gap <= REACH_STEPS) & even & (nj < block), 0.0, NEG)

        for slot_at in (A, C):
            @pl.when(sp < 2 - slot_at)
            def _():
                def clear(h, _):
                    ctx[h, :, :, slot_at] = jnp.zeros((2, CLASSES, class_rows, HEAD), BF16)
                    return 0
                lax.fori_loop(guests, heads, clear, 0)

        part_lse[...] = jnp.zeros(part_lse.shape, F32)
        back_lse[...] = jnp.zeros(back_lse.shape, F32)

        @pl.when(z == 0)
        def _():
            far_out[...] = jnp.zeros(far_out.shape, BF16)
            far_lse[...] = jnp.full(far_lse.shape, NEG, F32)
            mid_out[...] = jnp.zeros(mid_out.shape, BF16)
            mid_lse[...] = jnp.full(mid_lse.shape, NEG, F32)

    lane = iota((piece, HEAD), 1)
    low = lane < HEAD // 2
    power = (iota((1, HEAD), 1) % (HEAD // 2)).astype(F32)
    inverse = jnp.exp2(power * (-2.0 * float(np.log2(THETA_BASE)) / HEAD))

    def table(c, _):
        start = pl.multiple_of(c * piece, piece)
        places = start + iota((piece, HEAD), 0) + half_rows * jnp.where(low, tp, other)
        angles = (sp * rows + places).astype(F32) * inverse
        cosine, sine = jnp.cos(angles), jnp.sin(angles)
        cosine_moved, sine_moved = pltpu.roll(cosine, HEAD // 2, 1), pltpu.roll(sine, HEAD // 2, 1)
        own = pl.ds(pl.multiple_of(tp * half_rows + start, piece), piece)
        rest = pl.ds(pl.multiple_of(other * half_rows + start, piece), piece)
        cos_ref[own, :] = jnp.where(low, cosine, cosine_moved)
        sin_ref[own, :] = jnp.where(low, -sine, sine_moved)
        cos_ref[rest, :] = jnp.where(low, cosine_moved, cosine)
        sin_ref[rest, :] = jnp.where(low, -sine_moved, sine)
        return 0

    lax.fori_loop(0, PIECES, table, 0)
    q_copies[0].start()
    for kind in range(2):
        kv_copy(0, kind).start()

    def load_kv(h):
        pltpu.make_async_copy(wk_hbm.at[:, pl.ds(0, 2 * HEAD)], wkv.at[h], kv_sem.at[h]).wait()

    def raw_kv(source, h, count):
        kv = jnp.dot(source, wkv[h], preferred_element_type=F32)
        flat_a[0:count] = kv[:, :HEAD]
        flat_b[0:count] = kv[:, HEAD:]

    tok_copy.wait()

    pl.semaphore_wait(barrier, 2 + has_next.astype(jnp.int32) + (z > 0).astype(jnp.int32))

    x_copy = remote(x.at[tp], x.at[tp], x_sem.at[0], x_sem.at[1], across)
    x_copy.start()
    for h in (*range(guests + 1, heads), *range(1, guests)):
        for kind in range(2):
            kv_copy(h, kind).start()
    for copy in (*q_copies[1:], *wo_copies):
        copy.start()

    DOWN, SIDE, RELAY, ASK, SECOND, PART, MID, MIX = range(8)
    result_rows = (CLASSES * class_rows * HEAD // 2 + part_lse.shape[1] * HEAD) // HEAD

    def results(count, kind, arrived):
        both = num.at[pl.ds(0, count * result_rows)]
        return remote(both, both, sent.at[kind], arrived, down)

    def spots_of(half):
        return pl.ds(pl.multiple_of(half * half_class, half_class), half_class)

    def block_copy(h, src, dst, rows_at, kind, ids):
        arrived = a_recv.at[h - guests] if dst == A else c_recv.at[h]
        return remote(ctx.at[h, :, :, src, rows_at], ctx.at[h, :, :, dst, rows_at], sent.at[kind], arrived, ids)

    every = pl.ds(0, class_rows)

    def send_down(h, half):
        return ((has_next & (h >= guests), block_copy(jnp.maximum(h, guests), O, A, spots_of(half), DOWN, down)),)

    def send_side(h, half):
        return ((even | (h < guests), block_copy(h, O, C, spots_of(half), SIDE, side)),)

    def send_relay(h):
        return (((odd == 1) & (z > 0), block_copy(h, A, C, every, RELAY, side)),)

    def query_copy(h, half):
        rows_at, arrived = (spots_of(half), q_recv.at[2 * h + half]) if h < guests else (every, q_recv.at[guests + h])
        return remote(q.at[h, :, rows_at], visitor.at[h, :, rows_at], sent.at[ASK], arrived, up)

    def second_copy(h, rows_at):
        return remote(visitor.at[h, :, rows_at], second.at[h, :, rows_at], sent.at[SECOND], second_recv.at[h], up)

    def back_copies(h):
        return (remote(back.at[h], mid_out.at[h], sent.at[MID], mid_recv.at[h], down),
                remote(back_lse.at[h], mid_lse.at[h], sent.at[MID], mid_recv.at[h], down))

    def part_copies(h):
        return (remote(part.at[h], far_out.at[h], sent.at[PART], part_recv.at[h], down),
                remote(part_lse.at[h], far_lse.at[h], sent.at[PART], part_recv.at[h], down))

    def send_back(h):
        return tuple((has_second, copy) for copy in back_copies(h))

    def send_part(h):
        return tuple((has_next, copy) for copy in part_copies(h))

    def start_all(sends):
        for condition, copy in sends:
            @pl.when(condition)
            def _():
                copy.start()

    def project_kv(h, half):
        if half is None:
            source, natural, count, spots = x[...].reshape(rows, x.shape[2]), pl.ds(0, rows), rows, every
        else:
            source, natural = x[half], pl.ds(pl.multiple_of(half * half_rows, half_rows), half_rows)
            count, spots = half_rows, spots_of(half)
        raw_kv(source, h, count)
        k = rotated(flat_a[0:count], cos_ref[natural], sin_ref[natural])
        flat_a[0:count] = k
        kn[h, natural] = k.astype(BF16)
        vn[h, natural] = flat_b[0:count].astype(BF16)
        for c in range(CLASSES):
            ctx[h, 0, c, O, spots] = flat_a[classed(0, count // CLASSES, c), :].astype(BF16)
            ctx[h, 1, c, O, spots] = flat_b[classed(0, count // CLASSES, c), :].astype(BF16)
        for part_half in (order if half is None else (half,)):
            start_all(send_down(h, part_half))
            for condition, copy in send_side(h, part_half):
                @pl.when(h < guests)
                def _():
                    copy.start()

    def project_q(p, half):
        if half is None:
            source, natural, count = x[...].reshape(rows, x.shape[2]), pl.ds(0, rows), rows
            spots = pl.ds(0, class_rows)
        else:
            source, natural = x[half], pl.ds(pl.multiple_of(half * half_rows, half_rows), half_rows)
            count, spots = half_rows, pl.ds(pl.multiple_of(half * half_class, half_class), half_class)
        qq = jnp.dot(source, wq[p], preferred_element_type=F32)
        for s, flat in ((0, flat_a), (1, flat_b)):
            r = rotated(qq[:, s * HEAD:(s + 1) * HEAD], cos_ref[natural], sin_ref[natural])
            flat[0:count] = r
            qn[2 * p + s, natural] = r.astype(BF16)
            for c in range(CLASSES):
                q[2 * p + s, c, spots] = flat[classed(0, count // CLASSES, c), :].astype(BF16)

    def near(h, b, keys, vals, bias):
        scores = transposed_dot(qn[h, b * block:(b + 1) * block], keys) * SCALE + bias
        n, t, m = weighed(scores, vals)
        span = pl.ds(pl.multiple_of(h * rows, rows) + b * block, block)
        num[span, :] = n
        tot[span, :] = t
        top[span, :] = jnp.broadcast_to(m, (block, HEAD))

    def near_inner(h):
        for b in range(1, rows // block):
            span = slice((b - 1) * block, (b + 1) * block)
            near(h, b, kn[h, span], vn[h, span], band[1])

    def poll(h):
        @pl.when((odd == 1) & (z > 0))
        def _():
            block_copy(h, A, A, every, RELAY, side).wait_recv()
        start_all(send_relay(h))

    def meet(h, half):
        @pl.when(has_next)
        def _():
            query_copy(h, half).wait_recv()
        if h < guests:
            @pl.when(has_next & (z > 0))
            def _():
                second_copy(h, spots_of(half)).start()

    def neighbours(h):
        if h < guests:
            block_copy(h, C, C, every, SIDE, side).wait_recv()
        else:
            @pl.when(even & (z > 0))
            def _():
                block_copy(h, A, A, every, RELAY, side).wait_recv()

            @pl.when(sp > 0)
            def _():
                block_copy(h, C, C, every, SIDE, side).wait_recv()

    def mix_copy(h):
        return remote(mixg.at[2 * h + tp], mixg.at[2 * h + tp], sent.at[MIX], mix_recv.at[(h + 1) // heads], across)

    eye = iota((block, block), 0) == iota((block, block), 1)

    def context(h, c, kind, first, last):
        return ctx[h, kind, c, first:last].reshape((last - first) * class_rows, HEAD)

    def visit(h, guest, bias, first, last, result, lse):
        for c in range(CLASSES):
            keys, vals = (context(h, c, kind, first, last) for kind in range(2))
            n, t, m = weighed(transposed_dot(guest[h, c], keys) * SCALE + bias, vals)
            result[h, c] = (n / t).astype(BF16)
            lse[h, c:c + 1, :] = jnp.sum(jnp.where(eye, m + jnp.log2(t), 0.0), axis=0, keepdims=True)

    def visit_far(h):
        meet(h, 0)

        @pl.when(has_next)
        def _():
            visit(h, visitor, visit_bias[...], A, O, part, part_lse)
        start_all(send_part(h))

    def visit_second(h):
        @pl.when(has_second)
        def _():
            second_copy(h, every).wait_recv()
            visit(h, second, pair_bias[2], C, SLOTS, back, back_lse)
        start_all(send_back(h))

    def tail_of(h, kind):
        return [ctx[h, kind, c, C, class_rows - share:] for c in range(CLASSES)]

    def join(n, t, m, n2, t2, m2):
        most = jnp.maximum(m, m2)
        old, new = jnp.exp2(m - most), jnp.exp2(m2 - most)
        return n * old + n2 * new, t * old + t2 * new, most

    def visit_first(h):
        @pl.when(has_next)
        def _():
            keys, vals = (jnp.concatenate(tail_of(h, kind), axis=0) for kind in range(2))
            guest = jnp.concatenate([visitor[h, c, :share] for c in range(CLASSES)], axis=0)
            close = weighed(transposed_dot(guest, keys) * SCALE + band[3, :, :block], vals)
            for c in range(CLASSES):
                keys, vals = (context(h, c, kind, C, SLOTS) for kind in range(2))
                n, t, m = weighed(transposed_dot(visitor[h, c], keys) * SCALE + pair_bias[1], vals)
                m = jnp.broadcast_to(m, (block, HEAD))
                vnum[h, c], vtot[h, c], vtop[h, c] = n, t, m
                n, t, m = join(n[:share], t[:share], m[:share], *(v[c * share:(c + 1) * share] for v in close))
                vnum[h, c, :share], vtot[h, c, :share], vtop[h, c, :share] = n, t, m

    def with_far(n, t, m, result, lse_row):
        lf = jnp.sum(jnp.where(eye, lse_row, 0.0), axis=1, keepdims=True)
        most = jnp.maximum(m, lf)
        en, ef = jnp.exp2(m - most), jnp.exp2(lf - most)
        total = t * en + ef
        return (n * en + result.astype(F32) * ef) / total, total, most

    def merge(h):
        @pl.when(has_next)
        def _():
            @pl.when(z > 0)
            def _():
                results(1, MID, mid_recv.at[h]).wait_recv()
            for c in range(CLASSES):
                r, t, m = with_far(vnum[h, c], vtot[h, c], vtop[h, c], mid_out[h, c], mid_lse[h, c:c + 1, :])
                part[h, c] = r.astype(BF16)
                part_lse[h, c:c + 1, :] = jnp.sum(jnp.where(eye, m + jnp.log2(t), 0.0), axis=0, keepdims=True)
        start_all(send_part(h))

    def attend(h):
        first, bias, close = (C, pair_bias[0], band[2]) if h < guests else (A, far_bias[...], band[0])
        keys, vals = (jnp.concatenate(tail_of(h, kind) + [nat[h, :block]], axis=0)
                      for kind, nat in ((0, kn), (1, vn)))
        near(h, 0, keys, vals, close)
        for c in range(CLASSES):
            keys, vals = (context(h, c, kind, first, SLOTS) for kind in range(2))
            n, t, m = weighed(transposed_dot(q[h, c], keys) * SCALE + bias, vals)
            span = classed(h * rows, class_rows, c)
            cnum[h, c], ctot[h, c], ctop[h, c] = join(num[span, :], tot[span, :], top[span, :], n, t, m)

    def combine(h, _):
        @pl.when(z > 0)
        def _():
            results(1, PART, part_recv.at[h]).wait_recv()

        for c in range(CLASSES):
            mixed, _, _ = with_far(cnum[h, c], ctot[h, c], ctop[h, c], far_out[h, c], far_lse[h, pl.ds(c, 1), :])
            mixf[classed(0, class_rows, c), :] = mixed
        mixg[2 * h + tp] = mixf[...].astype(BF16)
        mix_copy(h).start()
        return 0

    def gathered(count, which):
        some = mixg.at[pl.ds(0, count)]
        remote(some, some, sent.at[MIX], mix_recv.at[which], across).wait_recv()

    out_cols = out_ref.shape[1]
    wide = 256

    def add_last(t, into):
        at = 2 * (heads - 1) + t
        span = pl.ds(pl.multiple_of(at * HEAD, HEAD), HEAD)
        for i in range(out_cols // wide):
            cols = pl.ds(i * wide, wide)
            total = jnp.dot(mixg[at], wo[span, cols], preferred_element_type=F32)
            into[:, cols] = (out_sum[:, cols] + total).astype(into.dtype)

    def partial_out():
        most = 2 * (heads - 1)
        mixed = jnp.concatenate([mixg[i] for i in range(most)], axis=1)
        for i in range(out_cols // wide):
            cols = pl.ds(i * wide, wide)
            out_sum[:, cols] = jnp.dot(mixed, wo[:most * HEAD, cols], preferred_element_type=F32)

    def ask(h, half):
        @pl.when(z > 0)
        def _():
            query_copy(h, half).start()

    load_kv(guests)
    project_kv(guests, tp)
    q_copies[0].wait()
    project_q(0, tp)
    for h in range(guests):
        ask(h, tp)
    load_kv(0)
    project_kv(0, tp)
    x_copy.wait_recv()
    project_kv(guests, other)
    project_q(0, other)
    ask(0, other)
    project_kv(0, other)

    def project_rest(i, _):
        late = heads - guests - 1
        h = jnp.where(i < late, guests + 1 + i, i - late + 1)
        load_kv(h)
        project_kv(h, None)
        for g in range(1, guests):
            @pl.when(i == g - 1)
            def _():
                ask(g, other)
        return 0

    lax.fori_loop(0, heads - 2, project_rest, 0)
    for h in range(guests, heads):
        for half in order:
            start_all(send_side(h, half))
    meet(0, tp)
    masks()
    meet(0, other)
    near_inner(0)
    near_inner(1)
    neighbours(0)
    for h in range(1, guests):
        meet(h, tp)
    visit_first(0)
    for h in range(1, guests):
        meet(h, other)
    poll(guests)
    attend(0)
    visit_second(0)
    for p in range(1, heads // 2):
        q_copies[p].wait()
        project_q(p, None)
    for h in range(guests, heads):
        ask(h, 0)
    for h in range(1, guests):
        poll(guests + h)
        near_inner(guests)
        neighbours(h)
        visit_second(h)
        visit_first(h)
        attend(h)
    for h in range(2 * guests, heads):
        poll(h)
    for h in range(guests + 1, heads):
        near_inner(h)
    for h in range(guests):
        merge(h)
    for h in range(guests, heads):
        neighbours(h)
        visit_far(h)
        attend(h)
        if h < heads - 1:
            combine(h - guests, 0)
    for h in range(heads - guests - 1, heads):
        combine(h, 0)
    pltpu.make_async_copy(wo_hbm, wo, wo_sem.at[0]).wait()
    gathered(heads - 1, 0)
    partial_out()
    add_last(tp, out_sum)
    gathered(1, 1)
    add_last(other, out_ref)

    x_copy.wait_send()
    firsts, rest = pl.ds(0, guests), pl.ds(guests, heads - guests)
    for condition, ref, kind in (
        (has_next, ctx.at[rest, :, :, O], DOWN),
        (even, ctx.at[:, :, :, O], SIDE),
        (odd == 1, ctx.at[firsts, :, :, O], SIDE),
        ((odd == 1) & (z > 0), ctx.at[rest, :, :, A], RELAY),
        (z > 0, q, ASK),
        (has_next & (z > 0), visitor.at[firsts], SECOND),
        (has_next, num.at[pl.ds(0, heads * result_rows)], PART),
        (has_second, num.at[pl.ds(0, guests * result_rows)], MID),
    ):
        @pl.when(condition)
        def _():
            remote(ref, ref, sent.at[kind], x_sem.at[1], side).wait_send()
    half_mix = mixg.at[pl.ds(0, heads)]
    remote(half_mix, half_mix, sent.at[MIX], x_sem.at[1], across).wait_send()


def body(tokens, query_weight, key_weight, value_weight, output_weight):
    n_sp = lax.axis_size("sp")
    half_rows, width = tokens.shape
    rows = half_rows * lax.axis_size("tp")
    heads = query_weight.shape[1] // HEAD
    assert rows * 4 == FAR_DILATION * REACH_STEPS and rows == 512
    assert n_sp % 2 == 0 and lax.axis_size("tp") == 2 and heads % 2 == 0 and heads >= 4

    guests = heads // 2
    class_rows = rows // CLASSES
    anywhere = pl.BlockSpec(memory_space=pl.ANY)
    vmem = pl.BlockSpec(memory_space=pltpu.VMEM)
    out_cols = output_weight.shape[1]
    dma = pltpu.SemaphoreType.DMA
    return pl.pallas_call(
        functools.partial(kernel, n_sp, heads, guests),
        out_shape=pltpu.VMEM((rows, out_cols), BF16),
        in_specs=[anywhere] * 5,
        out_specs=vmem,
        scratch_shapes=[
            pltpu.VMEM((2, half_rows, width), BF16),
            pltpu.VMEM((heads, width, 2 * HEAD), BF16),
            pltpu.VMEM((heads // 2, width, 2 * HEAD), BF16),
            pltpu.VMEM(output_weight.shape, BF16),
            pltpu.VMEM((rows, HEAD), F32),
            pltpu.VMEM((rows, HEAD), F32),
            pltpu.VMEM((heads, 2, CLASSES, SLOTS, class_rows, HEAD), BF16),
            pltpu.VMEM((heads, CLASSES, class_rows, HEAD), BF16),
            pltpu.VMEM((heads, rows, HEAD), BF16),
            pltpu.VMEM((heads, rows, HEAD), BF16),
            pltpu.VMEM((heads, rows, HEAD), BF16),
            pltpu.VMEM((heads, CLASSES, class_rows, HEAD), BF16),
            pltpu.VMEM((guests, CLASSES, class_rows, HEAD), BF16),
            pltpu.VMEM((rows, HEAD), F32),
            pltpu.VMEM((rows, HEAD), F32),
            pltpu.VMEM((REACH_STEPS, SLOTS * REACH_STEPS), F32),
            pltpu.VMEM((REACH_STEPS, 2 * REACH_STEPS), F32),
            pltpu.VMEM((3, REACH_STEPS, 2 * REACH_STEPS), F32),
            pltpu.VMEM((4, REACH_STEPS, 2 * REACH_STEPS), F32),
            pltpu.VMEM((heads * rows, HEAD), F32),
            pltpu.VMEM((heads * rows, HEAD), F32),
            pltpu.VMEM((heads * rows, HEAD), F32),
            pltpu.VMEM((heads, CLASSES, class_rows, HEAD), F32),
            pltpu.VMEM((heads, CLASSES, class_rows, HEAD), F32),
            pltpu.VMEM((heads, CLASSES, class_rows, HEAD), F32),
            pltpu.VMEM((guests, CLASSES, class_rows, HEAD), F32),
            pltpu.VMEM((guests, CLASSES, class_rows, HEAD), F32),
            pltpu.VMEM((guests, CLASSES, class_rows, HEAD), F32),
            pltpu.VMEM((heads, CLASSES, class_rows, HEAD), BF16),
            pltpu.VMEM((heads, 8, 128), F32),
            pltpu.VMEM((heads, CLASSES, class_rows, HEAD), BF16),
            pltpu.VMEM((heads, 8, 128), F32),
            pltpu.VMEM((guests, CLASSES, class_rows, HEAD), BF16),
            pltpu.VMEM((guests, 8, 128), F32),
            pltpu.VMEM((guests, CLASSES, class_rows, HEAD), BF16),
            pltpu.VMEM((guests, 8, 128), F32),
            pltpu.VMEM((rows, HEAD), F32),
            pltpu.VMEM((2 * heads, rows, HEAD), BF16),
            pltpu.VMEM((rows, out_cols), F32),
            dma((1,)),
            dma((heads,)),
            dma((heads // 2,)),
            dma((1,)),
            dma((2,)),
            dma((8,)),
            dma((heads - guests,)),
            dma((heads,)),
            dma((heads + guests,)),
            dma((guests,)),
            dma((heads,)),
            dma((guests,)),
            dma((2,)),
        ],
        compiler_params=pltpu.CompilerParams(
            collective_id=0, has_side_effects=True, vmem_limit_bytes=56 * 1024 * 1024
        ),
    )(tokens, query_weight, key_weight, value_weight, output_weight)


def solution(mesh):
    in_specs = (
        P(("grp", "sp", "tp"), None),
        P(None, "tp"),
        P(None, "tp"),
        P(None, "tp"),
        P(None, "tp"),
    )
    out_specs = P(("grp", "sp"), "tp")
    return jax.shard_map(body, mesh=mesh, in_specs=in_specs, out_specs=out_specs, check_vma=False)
```

```python
import functools

import jax
import jax.numpy as jnp
import numpy as np
from jax import lax
from jax.experimental import pallas as pl
from jax.experimental.pallas import tpu as pltpu
from jax.sharding import PartitionSpec as P

HEAD = 128
REACH_STEPS = 128
MIDDLE_DILATION = 4
FAR_DILATION = 16
THETA_BASE = 500000.0
NEG = -1e30
MESH = pl.DeviceIdType.MESH
F32 = jnp.float32
BF16 = jnp.bfloat16
SCALE = HEAD ** -0.5 / float(np.log(2.0))

A, C, O = 0, 1, 2
SLOTS = 3
CLASSES = MIDDLE_DILATION
PIECES = 2


def iota(shape, dim):
    return lax.broadcasted_iota(jnp.int32, shape, dim)


def rotated(x, cosine, sine):
    return x * cosine + pltpu.roll(x, HEAD // 2, 1) * sine


def weighed(scores, values):
    top = jnp.max(scores, axis=-1, keepdims=True)
    raised = jnp.exp2(scores - top).astype(BF16)
    ones = jnp.ones(values.shape, BF16)
    both = jnp.dot(raised, jnp.concatenate([values, ones], axis=1), preferred_element_type=F32)
    return both[:, :HEAD], both[:, HEAD:], top


def transposed_dot(a, b):
    return lax.dot_general(a, b, (((1,), (1,)), ((), ())), preferred_element_type=F32)


def classed(start, count, c):
    return pl.ds(start + c, count, stride=CLASSES)


def kernel(
    n_sp, heads, guests,
    tok_hbm, wq_hbm, wk_hbm, wv_hbm, wo_hbm,
    out_ref,
    x, wkv, wq, wo, cos_ref, sin_ref, ctx, q, qn, kn, vn, visitor, second, flat_a, flat_b,
    far_bias, visit_bias, pair_bias, band, num, tot, top, cnum, ctot, ctop, vnum, vtot, vtop,
    part, part_lse, far_out, far_lse, back, back_lse, mid_out, mid_lse, mixf, mixg, out_sum,
    tok_sem, kv_sem, q_load, wo_sem, x_sem, sent,
    a_recv, c_recv, q_recv, second_recv, part_recv, mid_recv, mix_recv,
):
    sp = lax.axis_index("sp")
    tp = lax.axis_index("tp")
    z = sp // 2
    odd = sp % 2
    even = odd == 0
    other = 1 - tp
    has_next = z + 1 < n_sp // 2
    has_second = z + 2 < n_sp // 2
    half_rows = x.shape[1]
    rows = 2 * half_rows
    class_rows = rows // CLASSES
    half_class = class_rows // 2
    piece = half_rows // PIECES
    order = (tp, other)

    tok_copy = pltpu.make_async_copy(tok_hbm, x.at[tp], tok_sem.at[0])
    tok_copy.start()

    def kv_copy(h, kind):
        source = (wk_hbm, wv_hbm)[kind]
        cols = pl.ds(h * HEAD, HEAD)
        return pltpu.make_async_copy(source.at[:, cols], wkv.at[h, :, pl.ds(kind * HEAD, HEAD)], kv_sem.at[h])

    q_copies = [
        pltpu.make_async_copy(wq_hbm.at[:, pl.ds(p * 2 * HEAD, 2 * HEAD)], wq.at[p], q_load.at[p])
        for p in range(heads // 2)]
    for kind in range(2):
        kv_copy(guests, kind).start()
    wo_copies = [
        pltpu.make_async_copy(
            wo_hbm.at[pl.ds((t * heads + h) * HEAD, HEAD)], wo.at[pl.ds((2 * h + t) * HEAD, HEAD)], wo_sem.at[0])
        for h in range(heads) for t in range(2)]

    barrier = pltpu.get_barrier_semaphore()
    y_partner = sp + 1 - 2 * odd

    def greet(ids):
        pl.semaphore_signal(barrier, inc=1, device_id=ids, device_id_type=MESH)

    greet({"tp": other})
    greet({"sp": y_partner})

    @pl.when(has_next)
    def _():
        greet({"sp": sp + 2})

    @pl.when(z > 0)
    def _():
        greet({"sp": sp - 2})

    def remote(src, dst, send_sem, recv_sem, ids):
        return pltpu.make_async_remote_copy(
            src_ref=src, dst_ref=dst, send_sem=send_sem, recv_sem=recv_sem,
            device_id=ids, device_id_type=MESH)

    down = {"sp": sp + 2}
    up = {"sp": sp - 2}
    side = {"sp": y_partner}
    across = {"tp": other}

    block = REACH_STEPS
    share = block // CLASSES
    ratio = FAR_DILATION // MIDDLE_DILATION

    def masks():
        qi, kj = iota((block, SLOTS * block), 0), iota((block, SLOTS * block), 1)
        slot = kj // block
        apart = qi - (kj % block)

        def bias(dist, here):
            steps = apart + block * dist
            mid = here & (steps >= 0) & (steps <= REACH_STEPS)
            far = here & (steps >= 0) & (steps % ratio == 0) & (steps <= ratio * REACH_STEPS)
            return jnp.where(mid & far, 1.0, jnp.where(mid | far, 0.0, NEG))

        far_bias[...] = bias(O - slot, O - slot <= sp)
        visit_bias[...] = bias(O + 2 - slot, O - slot <= sp)[:, :O * block]
        pair_bias[0] = bias(O - slot, (slot == O) | (odd == 1))[:, C * block:]
        pair_bias[1] = bias(jnp.where(slot == O, 2, 1 + 2 * odd), slot >= C)[:, C * block:]
        pair_bias[2] = bias(jnp.where(slot == O, 4, 3 + 2 * odd), slot >= C)[:, C * block:]
        ni, nj = iota((block, 2 * block), 0), iota((block, 2 * block), 1)
        gap = ni + block - nj
        band[1] = jnp.where((gap >= 0) & (gap <= REACH_STEPS), 0.0, NEG)
        gap = jnp.where(nj < block, ni + block - ((nj % share) * CLASSES + nj // share), gap)
        near_ok = (gap >= 0) & (gap <= REACH_STEPS)
        band[0] = jnp.where(near_ok & ((nj >= block) | (sp > 0)), 0.0, NEG)
        band[2] = jnp.where(near_ok & ((nj >= block) | (odd == 1)), 0.0, NEG)
        gap = ((ni % share) - (nj % share)) * CLASSES + ni // share - nj // share + block
        band[3] = jnp.where((gap >= 0) & (gap <= REACH_STEPS) & even & (nj < block), 0.0, NEG)

        for slot_at in (A, C):
            @pl.when(sp < 2 - slot_at)
            def _():
                def clear(h, _):
                    ctx[h, :, :, slot_at] = jnp.zeros((2, CLASSES, class_rows, HEAD), BF16)
                    return 0
                lax.fori_loop(guests, heads, clear, 0)

        part_lse[...] = jnp.zeros(part_lse.shape, F32)
        back_lse[...] = jnp.zeros(back_lse.shape, F32)

        @pl.when(z == 0)
        def _():
            far_out[...] = jnp.zeros(far_out.shape, BF16)
            far_lse[...] = jnp.full(far_lse.shape, NEG, F32)
            mid_out[...] = jnp.zeros(mid_out.shape, BF16)
            mid_lse[...] = jnp.full(mid_lse.shape, NEG, F32)

    lane = iota((piece, HEAD), 1)
    low = lane < HEAD // 2
    power = (iota((1, HEAD), 1) % (HEAD // 2)).astype(F32)
    inverse = jnp.exp2(power * (-2.0 * float(np.log2(THETA_BASE)) / HEAD))

    def table(c, _):
        start = pl.multiple_of(c * piece, piece)
        places = start + iota((piece, HEAD), 0) + half_rows * jnp.where(low, tp, other)
        angles = (sp * rows + places).astype(F32) * inverse
        cosine, sine = jnp.cos(angles), jnp.sin(angles)
        cosine_moved, sine_moved = pltpu.roll(cosine, HEAD // 2, 1), pltpu.roll(sine, HEAD // 2, 1)
        own = pl.ds(pl.multiple_of(tp * half_rows + start, piece), piece)
        rest = pl.ds(pl.multiple_of(other * half_rows + start, piece), piece)
        cos_ref[own, :] = jnp.where(low, cosine, cosine_moved)
        sin_ref[own, :] = jnp.where(low, -sine, sine_moved)
        cos_ref[rest, :] = jnp.where(low, cosine_moved, cosine)
        sin_ref[rest, :] = jnp.where(low, -sine_moved, sine)
        return 0

    lax.fori_loop(0, PIECES, table, 0)
    q_copies[0].start()
    for kind in range(2):
        kv_copy(0, kind).start()

    def load_kv(h):
        pltpu.make_async_copy(wk_hbm.at[:, pl.ds(0, 2 * HEAD)], wkv.at[h], kv_sem.at[h]).wait()

    def raw_kv(source, h, count):
        kv = jnp.dot(source, wkv[h], preferred_element_type=F32)
        flat_a[0:count] = kv[:, :HEAD]
        flat_b[0:count] = kv[:, HEAD:]

    tok_copy.wait()

    pl.semaphore_wait(barrier, 2 + has_next.astype(jnp.int32) + (z > 0).astype(jnp.int32))

    x_copy = remote(x.at[tp], x.at[tp], x_sem.at[0], x_sem.at[1], across)
    x_copy.start()
    for h in (*range(guests + 1, heads), *range(1, guests)):
        for kind in range(2):
            kv_copy(h, kind).start()
    for copy in (*q_copies[1:], *wo_copies):
        copy.start()

    DOWN, SIDE, RELAY, ASK, SECOND, PART, MID, MIX = range(8)
    result_rows = (CLASSES * class_rows * HEAD // 2 + part_lse.shape[1] * HEAD) // HEAD

    def results(count, kind, arrived):
        both = num.at[pl.ds(0, count * result_rows)]
        return remote(both, both, sent.at[kind], arrived, down)

    def spots_of(half):
        return pl.ds(pl.multiple_of(half * half_class, half_class), half_class)

    def block_copy(h, src, dst, rows_at, kind, ids):
        arrived = a_recv.at[h - guests] if dst == A else c_recv.at[h]
        return remote(ctx.at[h, :, :, src, rows_at], ctx.at[h, :, :, dst, rows_at], sent.at[kind], arrived, ids)

    every = pl.ds(0, class_rows)

    def send_down(h, half):
        return ((has_next & (h >= guests), block_copy(jnp.maximum(h, guests), O, A, spots_of(half), DOWN, down)),)

    def send_side(h, half):
        return ((even | (h < guests), block_copy(h, O, C, spots_of(half), SIDE, side)),)

    def send_relay(h):
        return (((odd == 1) & (z > 0), block_copy(h, A, C, every, RELAY, side)),)

    def query_copy(h, half):
        rows_at, arrived = (spots_of(half), q_recv.at[2 * h + half]) if h < guests else (every, q_recv.at[guests + h])
        return remote(q.at[h, :, rows_at], visitor.at[h, :, rows_at], sent.at[ASK], arrived, up)

    def second_copy(h, rows_at):
        return remote(visitor.at[h, :, rows_at], second.at[h, :, rows_at], sent.at[SECOND], second_recv.at[h], up)

    def back_copies(h):
        return (remote(back.at[h], mid_out.at[h], sent.at[MID], mid_recv.at[h], down),
                remote(back_lse.at[h], mid_lse.at[h], sent.at[MID], mid_recv.at[h], down))

    def part_copies(h):
        return (remote(part.at[h], far_out.at[h], sent.at[PART], part_recv.at[h], down),
                remote(part_lse.at[h], far_lse.at[h], sent.at[PART], part_recv.at[h], down))

    def send_back(h):
        return tuple((has_second, copy) for copy in back_copies(h))

    def send_part(h):
        return tuple((has_next, copy) for copy in part_copies(h))

    def start_all(sends):
        for condition, copy in sends:
            @pl.when(condition)
            def _():
                copy.start()

    def project_kv(h, half):
        if half is None:
            source, natural, count, spots = x[...].reshape(rows, x.shape[2]), pl.ds(0, rows), rows, every
        else:
            source, natural = x[half], pl.ds(pl.multiple_of(half * half_rows, half_rows), half_rows)
            count, spots = half_rows, spots_of(half)
        raw_kv(source, h, count)
        k = rotated(flat_a[0:count], cos_ref[natural], sin_ref[natural])
        flat_a[0:count] = k
        kn[h, natural] = k.astype(BF16)
        vn[h, natural] = flat_b[0:count].astype(BF16)
        for c in range(CLASSES):
            ctx[h, 0, c, O, spots] = flat_a[classed(0, count // CLASSES, c), :].astype(BF16)
            ctx[h, 1, c, O, spots] = flat_b[classed(0, count // CLASSES, c), :].astype(BF16)
        for part_half in (order if half is None else (half,)):
            start_all(send_down(h, part_half))
            for condition, copy in send_side(h, part_half):
                @pl.when(h < guests)
                def _():
                    copy.start()

    def project_q(p, half):
        if half is None:
            source, natural, count = x[...].reshape(rows, x.shape[2]), pl.ds(0, rows), rows
            spots = pl.ds(0, class_rows)
        else:
            source, natural = x[half], pl.ds(pl.multiple_of(half * half_rows, half_rows), half_rows)
            count, spots = half_rows, pl.ds(pl.multiple_of(half * half_class, half_class), half_class)
        qq = jnp.dot(source, wq[p], preferred_element_type=F32)
        for s, flat in ((0, flat_a), (1, flat_b)):
            r = rotated(qq[:, s * HEAD:(s + 1) * HEAD], cos_ref[natural], sin_ref[natural])
            flat[0:count] = r
            qn[2 * p + s, natural] = r.astype(BF16)
            for c in range(CLASSES):
                q[2 * p + s, c, spots] = flat[classed(0, count // CLASSES, c), :].astype(BF16)

    def near(h, b, keys, vals, bias):
        scores = transposed_dot(qn[h, b * block:(b + 1) * block], keys) * SCALE + bias
        n, t, m = weighed(scores, vals)
        span = pl.ds(pl.multiple_of(h * rows, rows) + b * block, block)
        num[span, :] = n
        tot[span, :] = t
        top[span, :] = jnp.broadcast_to(m, (block, HEAD))

    def near_inner(h):
        for b in range(1, rows // block):
            span = slice((b - 1) * block, (b + 1) * block)
            near(h, b, kn[h, span], vn[h, span], band[1])

    def poll(h):
        @pl.when((odd == 1) & (z > 0))
        def _():
            block_copy(h, A, A, every, RELAY, side).wait_recv()
        start_all(send_relay(h))

    def meet(h, half):
        @pl.when(has_next)
        def _():
            query_copy(h, half).wait_recv()
        if h < guests:
            @pl.when(has_next & (z > 0))
            def _():
                second_copy(h, spots_of(half)).start()

    def neighbours(h):
        if h < guests:
            block_copy(h, C, C, every, SIDE, side).wait_recv()
        else:
            @pl.when(even & (z > 0))
            def _():
                block_copy(h, A, A, every, RELAY, side).wait_recv()

            @pl.when(sp > 0)
            def _():
                block_copy(h, C, C, every, SIDE, side).wait_recv()

    def mix_copy(h):
        return remote(mixg.at[2 * h + tp], mixg.at[2 * h + tp], sent.at[MIX], mix_recv.at[(h + 1) // heads], across)

    eye = iota((block, block), 0) == iota((block, block), 1)

    def context(h, c, kind, first, last):
        return ctx[h, kind, c, first:last].reshape((last - first) * class_rows, HEAD)

    def visit(h, guest, bias, first, last, result, lse):
        for c in range(CLASSES):
            keys, vals = (context(h, c, kind, first, last) for kind in range(2))
            n, t, m = weighed(transposed_dot(guest[h, c], keys) * SCALE + bias, vals)
            result[h, c] = (n / t).astype(BF16)
            lse[h, c:c + 1, :] = jnp.sum(jnp.where(eye, m + jnp.log2(t), 0.0), axis=0, keepdims=True)

    def visit_far(h):
        meet(h, 0)

        @pl.when(has_next)
        def _():
            visit(h, visitor, visit_bias[...], A, O, part, part_lse)
        start_all(send_part(h))

    def visit_second(h):
        @pl.when(has_second)
        def _():
            second_copy(h, every).wait_recv()
            visit(h, second, pair_bias[2], C, SLOTS, back, back_lse)
        start_all(send_back(h))

    def tail_of(h, kind):
        return [ctx[h, kind, c, C, class_rows - share:] for c in range(CLASSES)]

    def join(n, t, m, n2, t2, m2):
        most = jnp.maximum(m, m2)
        old, new = jnp.exp2(m - most), jnp.exp2(m2 - most)
        return n * old + n2 * new, t * old + t2 * new, most

    def visit_first(h):
        @pl.when(has_next)
        def _():
            keys, vals = (jnp.concatenate(tail_of(h, kind), axis=0) for kind in range(2))
            guest = jnp.concatenate([visitor[h, c, :share] for c in range(CLASSES)], axis=0)
            close = weighed(transposed_dot(guest, keys) * SCALE + band[3, :, :block], vals)
            for c in range(CLASSES):
                keys, vals = (context(h, c, kind, C, SLOTS) for kind in range(2))
                n, t, m = weighed(transposed_dot(visitor[h, c], keys) * SCALE + pair_bias[1], vals)
                m = jnp.broadcast_to(m, (block, HEAD))
                vnum[h, c], vtot[h, c], vtop[h, c] = n, t, m
                n, t, m = join(n[:share], t[:share], m[:share], *(v[c * share:(c + 1) * share] for v in close))
                vnum[h, c, :share], vtot[h, c, :share], vtop[h, c, :share] = n, t, m

    def with_far(n, t, m, result, lse_row):
        lf = jnp.sum(jnp.where(eye, lse_row, 0.0), axis=1, keepdims=True)
        most = jnp.maximum(m, lf)
        en, ef = jnp.exp2(m - most), jnp.exp2(lf - most)
        total = t * en + ef
        return (n * en + result.astype(F32) * ef) / total, total, most

    def merge(h):
        @pl.when(has_next)
        def _():
            @pl.when(z > 0)
            def _():
                results(1, MID, mid_recv.at[h]).wait_recv()
            for c in range(CLASSES):
                r, t, m = with_far(vnum[h, c], vtot[h, c], vtop[h, c], mid_out[h, c], mid_lse[h, c:c + 1, :])
                part[h, c] = r.astype(BF16)
                part_lse[h, c:c + 1, :] = jnp.sum(jnp.where(eye, m + jnp.log2(t), 0.0), axis=0, keepdims=True)
        start_all(send_part(h))

    def attend(h):
        first, bias, close = (C, pair_bias[0], band[2]) if h < guests else (A, far_bias[...], band[0])
        keys, vals = (jnp.concatenate(tail_of(h, kind) + [nat[h, :block]], axis=0)
                      for kind, nat in ((0, kn), (1, vn)))
        near(h, 0, keys, vals, close)
        for c in range(CLASSES):
            keys, vals = (context(h, c, kind, first, SLOTS) for kind in range(2))
            n, t, m = weighed(transposed_dot(q[h, c], keys) * SCALE + bias, vals)
            span = classed(h * rows, class_rows, c)
            cnum[h, c], ctot[h, c], ctop[h, c] = join(num[span, :], tot[span, :], top[span, :], n, t, m)

    def combine(h, _):
        @pl.when(z > 0)
        def _():
            results(1, PART, part_recv.at[h]).wait_recv()

        for c in range(CLASSES):
            mixed, _, _ = with_far(cnum[h, c], ctot[h, c], ctop[h, c], far_out[h, c], far_lse[h, pl.ds(c, 1), :])
            mixf[classed(0, class_rows, c), :] = mixed
        mixg[2 * h + tp] = mixf[...].astype(BF16)
        mix_copy(h).start()
        return 0

    def gathered(count, which):
        some = mixg.at[pl.ds(0, count)]
        remote(some, some, sent.at[MIX], mix_recv.at[which], across).wait_recv()

    out_cols = out_ref.shape[1]
    wide = 256

    def add_last(t, into):
        at = 2 * (heads - 1) + t
        span = pl.ds(pl.multiple_of(at * HEAD, HEAD), HEAD)
        for i in range(out_cols // wide):
            cols = pl.ds(i * wide, wide)
            total = jnp.dot(mixg[at], wo[span, cols], preferred_element_type=F32)
            into[:, cols] = (out_sum[:, cols] + total).astype(into.dtype)

    def partial_out():
        most = 2 * (heads - 1)
        mixed = jnp.concatenate([mixg[i] for i in range(most)], axis=1)
        for i in range(out_cols // wide):
            cols = pl.ds(i * wide, wide)
            out_sum[:, cols] = jnp.dot(mixed, wo[:most * HEAD, cols], preferred_element_type=F32)

    def ask(h, half):
        @pl.when(z > 0)
        def _():
            query_copy(h, half).start()

    load_kv(guests)
    project_kv(guests, tp)
    q_copies[0].wait()
    project_q(0, tp)
    for h in range(guests):
        ask(h, tp)
    load_kv(0)
    project_kv(0, tp)
    x_copy.wait_recv()
    project_q(0, other)
    ask(0, other)
    project_kv(guests, other)
    project_kv(0, other)

    def project_rest(i, _):
        late = heads - guests - 1
        h = jnp.where(i < late, guests + 1 + i, i - late + 1)
        load_kv(h)
        project_kv(h, None)
        for g in range(1, guests):
            @pl.when(i == g - 1)
            def _():
                ask(g, other)
        return 0

    lax.fori_loop(0, heads - 2, project_rest, 0)
    for h in range(guests, heads):
        for half in order:
            start_all(send_side(h, half))
    meet(0, tp)
    masks()
    meet(0, other)
    near_inner(0)
    near_inner(1)
    neighbours(0)
    for h in range(1, guests):
        meet(h, tp)
    visit_first(0)
    for h in range(1, guests):
        meet(h, other)
    poll(guests)
    attend(0)
    visit_second(0)
    for p in range(1, heads // 2):
        q_copies[p].wait()
        project_q(p, None)
    for h in range(guests, heads):
        ask(h, 0)
    for h in range(1, guests):
        poll(guests + h)
        near_inner(guests)
        neighbours(h)
        visit_second(h)
        visit_first(h)
        attend(h)
    for h in range(2 * guests, heads):
        poll(h)
    for h in range(guests + 1, heads):
        near_inner(h)
    for h in range(guests):
        merge(h)
    for h in range(guests, heads):
        neighbours(h)
        visit_far(h)
        attend(h)
        if h < heads - 1:
            combine(h - guests, 0)
    for h in range(heads - guests - 1, heads):
        combine(h, 0)
    pltpu.make_async_copy(wo_hbm, wo, wo_sem.at[0]).wait()
    gathered(heads - 1, 0)
    partial_out()
    add_last(tp, out_sum)
    gathered(1, 1)
    add_last(other, out_ref)

    x_copy.wait_send()
    firsts, rest = pl.ds(0, guests), pl.ds(guests, heads - guests)
    for condition, ref, kind in (
        (has_next, ctx.at[rest, :, :, O], DOWN),
        (even, ctx.at[:, :, :, O], SIDE),
        (odd == 1, ctx.at[firsts, :, :, O], SIDE),
        ((odd == 1) & (z > 0), ctx.at[rest, :, :, A], RELAY),
        (z > 0, q, ASK),
        (has_next & (z > 0), visitor.at[firsts], SECOND),
        (has_next, num.at[pl.ds(0, heads * result_rows)], PART),
        (has_second, num.at[pl.ds(0, guests * result_rows)], MID),
    ):
        @pl.when(condition)
        def _():
            remote(ref, ref, sent.at[kind], x_sem.at[1], side).wait_send()
    half_mix = mixg.at[pl.ds(0, heads)]
    remote(half_mix, half_mix, sent.at[MIX], x_sem.at[1], across).wait_send()


def body(tokens, query_weight, key_weight, value_weight, output_weight):
    n_sp = lax.axis_size("sp")
    half_rows, width = tokens.shape
    rows = half_rows * lax.axis_size("tp")
    heads = query_weight.shape[1] // HEAD
    assert rows * 4 == FAR_DILATION * REACH_STEPS and rows == 512
    assert n_sp % 2 == 0 and lax.axis_size("tp") == 2 and heads % 2 == 0 and heads >= 4

    guests = heads // 2
    class_rows = rows // CLASSES
    anywhere = pl.BlockSpec(memory_space=pl.ANY)
    vmem = pl.BlockSpec(memory_space=pltpu.VMEM)
    out_cols = output_weight.shape[1]
    dma = pltpu.SemaphoreType.DMA
    return pl.pallas_call(
        functools.partial(kernel, n_sp, heads, guests),
        out_shape=pltpu.VMEM((rows, out_cols), BF16),
        in_specs=[anywhere] * 5,
        out_specs=vmem,
        scratch_shapes=[
            pltpu.VMEM((2, half_rows, width), BF16),
            pltpu.VMEM((heads, width, 2 * HEAD), BF16),
            pltpu.VMEM((heads // 2, width, 2 * HEAD), BF16),
            pltpu.VMEM(output_weight.shape, BF16),
            pltpu.VMEM((rows, HEAD), F32),
            pltpu.VMEM((rows, HEAD), F32),
            pltpu.VMEM((heads, 2, CLASSES, SLOTS, class_rows, HEAD), BF16),
            pltpu.VMEM((heads, CLASSES, class_rows, HEAD), BF16),
            pltpu.VMEM((heads, rows, HEAD), BF16),
            pltpu.VMEM((heads, rows, HEAD), BF16),
            pltpu.VMEM((heads, rows, HEAD), BF16),
            pltpu.VMEM((heads, CLASSES, class_rows, HEAD), BF16),
            pltpu.VMEM((guests, CLASSES, class_rows, HEAD), BF16),
            pltpu.VMEM((rows, HEAD), F32),
            pltpu.VMEM((rows, HEAD), F32),
            pltpu.VMEM((REACH_STEPS, SLOTS * REACH_STEPS), F32),
            pltpu.VMEM((REACH_STEPS, 2 * REACH_STEPS), F32),
            pltpu.VMEM((3, REACH_STEPS, 2 * REACH_STEPS), F32),
            pltpu.VMEM((4, REACH_STEPS, 2 * REACH_STEPS), F32),
            pltpu.VMEM((heads * rows, HEAD), F32),
            pltpu.VMEM((heads * rows, HEAD), F32),
            pltpu.VMEM((heads * rows, HEAD), F32),
            pltpu.VMEM((heads, CLASSES, class_rows, HEAD), F32),
            pltpu.VMEM((heads, CLASSES, class_rows, HEAD), F32),
            pltpu.VMEM((heads, CLASSES, class_rows, HEAD), F32),
            pltpu.VMEM((guests, CLASSES, class_rows, HEAD), F32),
            pltpu.VMEM((guests, CLASSES, class_rows, HEAD), F32),
            pltpu.VMEM((guests, CLASSES, class_rows, HEAD), F32),
            pltpu.VMEM((heads, CLASSES, class_rows, HEAD), BF16),
            pltpu.VMEM((heads, 8, 128), F32),
            pltpu.VMEM((heads, CLASSES, class_rows, HEAD), BF16),
            pltpu.VMEM((heads, 8, 128), F32),
            pltpu.VMEM((guests, CLASSES, class_rows, HEAD), BF16),
            pltpu.VMEM((guests, 8, 128), F32),
            pltpu.VMEM((guests, CLASSES, class_rows, HEAD), BF16),
            pltpu.VMEM((guests, 8, 128), F32),
            pltpu.VMEM((rows, HEAD), F32),
            pltpu.VMEM((2 * heads, rows, HEAD), BF16),
            pltpu.VMEM((rows, out_cols), F32),
            dma((1,)),
            dma((heads,)),
            dma((heads // 2,)),
            dma((1,)),
            dma((2,)),
            dma((8,)),
            dma((heads - guests,)),
            dma((heads,)),
            dma((heads + guests,)),
            dma((guests,)),
            dma((heads,)),
            dma((guests,)),
            dma((2,)),
        ],
        compiler_params=pltpu.CompilerParams(
            collective_id=0, has_side_effects=True, vmem_limit_bytes=56 * 1024 * 1024
        ),
    )(tokens, query_weight, key_weight, value_weight, output_weight)


def solution(mesh):
    in_specs = (
        P(("grp", "sp", "tp"), None),
        P(None, "tp"),
        P(None, "tp"),
        P(None, "tp"),
        P(None, "tp"),
    )
    out_specs = P(("grp", "sp"), "tp")
    return jax.shard_map(body, mesh=mesh, in_specs=in_specs, out_specs=out_specs, check_vma=False)
```
